32 devices in a mesh: sp: 16 (over z, y, x), tp: 2 (over core).
Axes of the slice: x: 2, y: 2, z: 4, core: 2. Of those that a mesh axis runs over, the one named last changes fastest.
Arguments:
- prompt: bfloat16 [2, 3072, 4096], P(None, 'sp'), as said below
- w_key: bfloat16 [4096, 2048], P('sp', 'tp'), may hold values from -0.09375 to 0.09375
- w_value: bfloat16 [4096, 4096], P('sp', 'tp'), may hold values from -0.09375 to 0.09375
- w_igate: bfloat16 [4096, 8], replicated, may hold values from -0.09375 to 0.09375
- w_fgate: bfloat16 [4096, 8], replicated, may hold values from -0.09375 to 0.09375
- input_bias: float32 [8], replicated, may hold values from -1 to 120
- forget_bias: float32 [8], replicated, may hold values from 4 to 20
- new_query: bfloat16 [2, 8, 256], P(None, 'tp'), may hold values from -6 to 6
- new_key: bfloat16 [2, 8, 256], P(None, 'tp'), may hold values from -6 to 6
- new_value: bfloat16 [2, 8, 512], P(None, 'tp'), may hold values from -6 to 6
- new_gates: float32 [2, 2, 8], P(None, None, 'tp'), may hold values from 2 to 9
Outputs:
- cache_memory: bfloat16 [2, 8, 256, 512], P(None, 'tp', 'sp')
- cache_norm: float32 [2, 8, 256], P(None, 'tp', 'sp')
- cache_max: float32 [2, 8], P(None, 'tp')
- first_read: bfloat16 [2, 8, 512], P(None, 'tp')
The draws below stay inside these ranges and needn't reach their ends.
Inputs may be any that keep to these rules, and one draw needn't show every extreme that they name: `prompt`: Real-valued features, each entry drawn independently; their magnitude differs from one block of 192 positions to the next.
All inputs are finite; a program needn't handle non-finite values.
Results may differ from the reference program's by a relative error of at most 0.019.
Values may be sent and summed in bfloat16 or wider, within the bound.
A program may use at most 64 MiB of HBM per device.

```python
import math
import jax
import jax.numpy as jnp
from jax import lax

D = 4096
HEADS = 8
DK = 256
DV = 512
SEQS = 2
SPAN = 192
LEN = 3072


def draw_prompt(key, part):
    first, second = jax.random.split(jax.random.fold_in(key, 11))
    base = jax.random.normal(first, (SEQS, LEN // SPAN, SPAN, D), jnp.float32)
    lower, upper = (0.6, 1.7)
    scales = jnp.exp(jax.random.uniform(second, (SEQS, LEN // SPAN, 1, 1), jnp.float32, math.log(lower), math.log(upper)))
    return (base * scales).reshape(SEQS, LEN, D).astype(jnp.bfloat16)


def draw_input_bias(key, part):
    inner = jax.random.fold_in(key, 23)
    return jax.random.uniform(inner, (HEADS,), jnp.float32, -1.0, 1.0)


def draw_forget_bias(key, part):
    first, second, third = jax.random.split(jax.random.fold_in(key, 37), 3)
    picks = jax.random.randint(first, (HEADS,), 0, 8)
    quick = picks < 4
    slow_value = math.log(float(LEN)) + jax.random.uniform(second, (HEADS,), jnp.float32, 1.5, 2.5)
    quick_value = jax.random.uniform(third, (HEADS,), jnp.float32, 4.0, 5.0)
    return jnp.where(quick, quick_value, slow_value)


def shard_levels(own_key, dims, cuts, least, top_value):
    level = 1.0
    for position, parts in cuts:
        heights = jax.random.uniform(jax.random.fold_in(jax.random.fold_in(own_key, 6), position), (parts,), jnp.float32, least / len(cuts), top_value / len(cuts))
        level = level * jnp.repeat(jnp.exp(heights), dims[position] // parts).reshape((-1,) + (1,) * (len(dims) - 1 - position))
    return level


def normal_values(own_key, dims, deviation, limit, shards=(), held_as=jnp.bfloat16):
    result = deviation * jax.random.normal(own_key, dims, jnp.float32)
    if shards:
        result = result * shard_levels(own_key, dims, shards, -0.22, 0.18)
    return jnp.clip(result, -limit, limit).astype(held_as)


def setup_inputs(seed: int = 0) -> dict:
    key_list = jax.random.split(jax.random.key(seed), 12)
    prompt = draw_prompt(jax.random.fold_in(key_list[11], 71), 0)
    w_key = normal_values(key_list[1], (D, HEADS * DK), D ** -0.5, 0.09375, ((0, 16), (1, 2)))
    w_value = normal_values(key_list[2], (D, HEADS * DV), D ** -0.5, 0.09375, ((0, 16), (1, 2)))
    w_igate = normal_values(key_list[3], (D, HEADS), D ** -0.5, 0.09375)
    w_fgate = normal_values(key_list[4], (D, HEADS), D ** -0.5, 0.09375)
    input_bias = draw_input_bias(jax.random.fold_in(key_list[11], 71), 0)
    forget_bias = draw_forget_bias(jax.random.fold_in(key_list[11], 71), 0)
    new_query = normal_values(key_list[7], (SEQS, HEADS, DK), 1.0, 6.0, ((1, 2),))
    new_key = normal_values(key_list[8], (SEQS, HEADS, DK), 1.0, 6.0, ((1, 2),))
    new_value = normal_values(key_list[9], (SEQS, HEADS, DV), 1.0, 6.0, ((1, 2),))
    new_gates = jnp.clip(2.0 + 7.0 * jax.random.uniform(key_list[10], (2, SEQS, HEADS), jnp.float32) ** shard_levels(key_list[10], (2, SEQS, HEADS), ((2, 2),), -0.2, 0.2), 2.0, 9.0)
    return {"prompt": prompt, "w_key": w_key, "w_value": w_value, "w_igate": w_igate, "w_fgate": w_fgate, "input_bias": input_bias, "forget_bias": forget_bias, "new_query": new_query, "new_key": new_key, "new_value": new_value, "new_gates": new_gates}


def reference(prompt, w_key, w_value, w_igate, w_fgate, input_bias, forget_bias, new_query, new_key, new_value, new_gates):
    blocks = LEN // SPAN
    token_rows = prompt.reshape(SEQS * LEN, D)
    key_rows = jnp.dot(token_rows, w_key, preferred_element_type=jnp.float32).astype(jnp.bfloat16)
    value_rows = jnp.dot(token_rows, w_value, preferred_element_type=jnp.float32).astype(jnp.bfloat16)
    input_gate = jnp.dot(token_rows, w_igate, preferred_element_type=jnp.float32) + input_bias
    log_forget = jax.nn.log_sigmoid(jnp.dot(token_rows, w_fgate, preferred_element_type=jnp.float32) + forget_bias)
    input_gate = input_gate.reshape(SEQS, blocks, SPAN, HEADS)
    log_forget = log_forget.reshape(SEQS, blocks, SPAN, HEADS)
    block_total = jnp.sum(log_forget, axis=2)
    forget_after = block_total[:, :, None] - jnp.cumsum(log_forget, axis=2)
    log_weight = forget_after + input_gate
    block_max = jnp.max(log_weight, axis=2)
    later_total = jnp.flip(jnp.cumsum(jnp.flip(block_total, 1), axis=1), 1) - block_total
    block_lift = later_total + block_max
    global_max = jnp.max(block_lift, axis=1)
    factor = jnp.exp(block_lift - global_max[:, None])
    key_scale = DK ** -0.5
    key_blocks = key_rows.reshape(SEQS, blocks, SPAN, HEADS, DK).astype(jnp.float32)
    decayed = (jnp.exp(log_weight - block_max[:, :, None])[..., None] * key_scale * key_blocks).astype(jnp.bfloat16)
    value_blocks = value_rows.reshape(SEQS, blocks, SPAN, HEADS, DV)

    def accumulate(carry, inputs):
        memory, normal = carry
        block_keys, block_values, block_factor = inputs
        block_state = jnp.einsum('sthk,sthv->shkv', block_keys.astype(jnp.float32), block_values.astype(jnp.float32),
                                 precision=lax.Precision.HIGHEST)
        block_norm = jnp.sum(block_keys.astype(jnp.float32), axis=1)
        memory = memory + block_factor[:, :, None, None] * block_state
        normal = normal + block_factor[:, :, None] * block_norm
        return (memory, normal), None

    inputs = (jnp.moveaxis(decayed, 1, 0), jnp.moveaxis(value_blocks, 1, 0), jnp.moveaxis(factor, 1, 0))
    start = (jnp.zeros((SEQS, HEADS, DK, DV), jnp.float32), jnp.zeros((SEQS, HEADS, DK), jnp.float32))
    (memory, normal), _ = lax.scan(accumulate, start, inputs)
    query_full = new_query.astype(jnp.float32)
    query_state = jnp.einsum('shk,shkv->shv', query_full, memory, precision=lax.Precision.HIGHEST)
    query_norm = jnp.sum(query_full * normal, axis=-1)
    forget_new = jax.nn.log_sigmoid(new_gates[1])
    input_new = new_gates[0]
    mixed = jnp.maximum(forget_new + global_max, input_new)
    carried = jnp.exp(forget_new + global_max - mixed)
    fresh = jnp.exp(input_new - mixed)
    own_score = jnp.sum(query_full * new_key.astype(jnp.float32), axis=-1) * key_scale
    numer = carried[..., None] * query_state + (fresh * own_score)[..., None] * new_value.astype(jnp.float32)
    denom = carried * query_norm + fresh * own_score
    first_read = (numer / jnp.maximum(jnp.abs(denom), 1.0)[..., None]).astype(jnp.bfloat16)
    return memory.astype(jnp.bfloat16), normal, global_max, first_read
```

```python
import functools
import jax
import jax.numpy as jnp
from jax import lax
from jax.experimental import pallas as pl
from jax.experimental.pallas import tpu as pltpu
from jax.sharding import PartitionSpec as P

HIGH = lax.Precision.HIGHEST
UNITS = 8
SENDS = 160


def flip(bit, change):
    return bit + change - 2 * bit * change


def log_sigmoid(v):
    return jnp.minimum(v, 0.0) - jnp.log1p(jnp.exp(-jnp.abs(v)))


def iota(shape, dim):
    return lax.broadcasted_iota(jnp.int32, shape, dim)


def kernel(
    prompt,
    w_key,
    w_value,
    w_igate,
    w_fgate,
    input_bias,
    forget_bias,
    new_query,
    new_key,
    new_value,
    new_gates,
    memory_out,
    norm_out,
    max_out,
    read_out,
    xb,
    wb,
    pass_w,
    acc,
    decay,
    vals,
    weight,
    gate_w,
    stat,
    state,
    aux,
    rmem,
    raux,
    local_sem,
    sends,
    x_recv,
    d_recv,
    w_recv,
    g_recv,
    s_recv,
    m_recv,
    a_recv,
):
    count = lax.axis_size("sp")
    me = lax.axis_index("sp")
    core = lax.axis_index("tp")
    seqs, span, width = prompt.shape
    depth = w_key.shape[0]
    heads = new_query.shape[1]
    dk = new_query.shape[2]
    dv = new_value.shape[2]
    total_heads = input_bias.shape[1]
    key_scale = dk ** (-0.5)
    per_seq = UNITS // seqs
    cut = width // (2 * per_seq)
    rows_out = dk // count
    zh, zl, y, x = me // 8, (me // 4) % 2, (me // 2) % 2, me % 2
    mine = zl * 2 + x
    inner = zh != zl
    bf16, f32 = jnp.bfloat16, jnp.float32

    def place(dh, dl, dy, dx):
        return flip(zh, dh) * 8 + flip(zl, dl) * 4 + flip(y, dy) * 2 + flip(x, dx)

    sent = []

    def remote(src, dst, recv, sp, tp, when=None):
        copy = pltpu.make_async_remote_copy(
            src_ref=src,
            dst_ref=dst,
            send_sem=sends.at[len(sent)],
            recv_sem=recv,
            device_id=(sp, tp),
            device_id_type=pl.DeviceIdType.MESH,
        )
        sent.append((copy, when))
        return copy

    def start(copies, when=None):
        def run():
            for copy in copies:
                copy.start()

        if when is None:
            run()
        else:
            pl.when(when)(run)

    def landed(ref, sem):
        pltpu.make_async_copy(ref, ref, sem).wait()

    barrier = pltpu.get_barrier_semaphore()
    for off in range(1, count):
        pl.semaphore_signal(
            barrier,
            inc=1,
            device_id=((me + off) % count, core),
            device_id_type=pl.DeviceIdType.MESH,
        )
    pl.semaphore_signal(
        barrier, inc=1, device_id=(me, 1 - core), device_id_type=pl.DeviceIdType.MESH
    )

    def bits(slot):
        return slot // 8, (slot // 4) % 2, (slot // 2) % 2, slot % 2

    def w_rows(slot):
        return pl.ds(pl.multiple_of(place(*bits(slot)) * depth, depth), depth)

    def group_cols(dl, dx):
        group = flip(zl, dl) * 2 + flip(x, dx)
        kc = pl.ds(pl.multiple_of(group * dk, dk), dk)
        vc = pl.ds(pl.multiple_of(group * dv, dv), dv)
        return kc, vc

    own_x = []
    for s in range(seqs):
        c = pltpu.make_async_copy(
            prompt.at[s], xb.at[0, pl.ds(s * span, span)], local_sem.at[s]
        )
        c.start()
        own_x.append(c)
    kc, vc = group_cols(0, 0)
    own_w = [
        pltpu.make_async_copy(w_key.at[:, kc], wb.at[w_rows(0), :dk], local_sem.at[2]),
        pltpu.make_async_copy(w_value.at[:, vc], wb.at[w_rows(0), dk:], local_sem.at[3]),
    ]
    for c in own_w:
        c.start()
    pl.semaphore_wait(barrier, count)

    to_x, to_y, to_z = place(0, 0, 0, 1), place(0, 0, 1, 0), place(0, 1, 0, 0)
    to_far, to_mid = place(1, 0, 0, 0), place(1, 1, 0, 0)

    def w_own(dl, dx, peer, slot, when=None):
        kc, vc = group_cols(dl, dx)
        rows = w_rows(0)
        return [
            remote(w_key.at[:, kc], wb.at[rows, :dk], w_recv.at[slot], peer, core, when),
            remote(w_value.at[:, vc], wb.at[rows, dk:], w_recv.at[slot], peer, core, when),
        ]

    def w_relay(slot, peer, there, when=None):
        rows = w_rows(slot)
        return [remote(wb.at[rows], wb.at[rows], w_recv.at[there], peer, core, when)]

    def w_wait(slot):
        landed(wb.at[w_rows(slot)], w_recv.at[slot])

    def part(block, unit, owner):
        s, k = unit // per_seq, unit % per_seq
        cols = pl.ds(pl.multiple_of((owner * per_seq + k) * cut, cut), cut)
        return xb.at[block, pl.ds(s * span, span), cols]

    def x_own(block, unit, peer):
        s, k = unit // per_seq, unit % per_seq
        cols = pl.ds(pl.multiple_of((core * per_seq + k) * cut, cut), cut)
        return [
            remote(
                prompt.at[s, :, cols],
                part(block, unit, core),
                x_recv.at[block, unit],
                peer,
                core,
            )
        ]

    def x_relay(unit):
        return [
            remote(part(2, unit, core), part(3, unit, core), x_recv.at[3, unit], to_x, core)
        ]

    def x_across(block, unit):
        own = part(block, unit, core)
        return [remote(own, own, d_recv.at[block, unit], me, 1 - core)]

    def x_wait(block, unit):
        landed(part(block, unit, core), x_recv.at[block, unit])

    def d_wait(block, unit):
        landed(part(block, unit, 1 - core), d_recv.at[block, unit])

    def go_x(block, units):
        for unit in units:
            x_wait(block, unit)
            if block == 2:
                start(x_relay(unit))
            start(x_across(block, unit))

    def d_all(block, s):
        for unit in range(s * per_seq, (s + 1) * per_seq):
            d_wait(block, unit)

    def go_w(slot):
        w_wait(slot)
        start(w_relay(slot, to_y, slot + 2))

    first = core == 0

    near, far, mid = (
        w_own(1, 0, to_z, 4),
        w_own(0, 0, to_far, 8),
        w_own(1, 0, to_mid, 12, inner),
    )
    tokens = [x_own(2, unit, to_z) for unit in range(UNITS)]
    px = w_own(0, 1, to_x, 1)
    kc, vc = group_cols(1, 1)
    px2 = [
        remote(w_key.at[:, kc], pass_w.at[:, :dk], w_recv.at[0], to_x, core),
        remote(w_value.at[:, vc], pass_w.at[:, dk:], w_recv.at[0], to_x, core),
    ]
    start(px)
    start(w_own(0, 0, to_y, 2))

    @pl.when(first)
    def _():
        start(far)
        start(near)

    @pl.when(core == 1)
    def _():
        start(near)
        start(far)

    start(px2)
    start(mid, inner)
    for unit in range(2):
        start(tokens[unit])
    for unit in range(UNITS):
        start(x_own(1, unit, to_x))

    w_gate = jnp.concatenate([w_igate[...], w_fgate[...]], axis=0)
    square = iota((total_heads, total_heads), 0) == iota((total_heads, total_heads), 1)

    def upright(row):
        return jnp.sum(jnp.where(square, row, 0.0), axis=1, keepdims=True)

    bias_in, bias_f = upright(input_bias[...]), upright(forget_bias[...])
    after = (iota((span, span), 0) > iota((span, span), 1)).astype(f32)
    spot_head = iota((total_heads, 128), 0) - core * heads
    spot_lane = iota((total_heads, 128), 1)
    local_head = (spot_head >= 0) & (spot_head < heads)
    for c in own_x:
        c.wait()
    packed = jnp.zeros((1, 128), f32)
    gate_w[0] = jnp.zeros(gate_w.shape[1:], f32)
    for s in range(seqs):
        both = lax.dot_general(
            w_gate,
            xb[0, s * span : (s + 1) * span],
            (((1,), (1,)), ((), ())),
            preferred_element_type=f32,
        )
        gate_in = both[:total_heads] + bias_in
        forget = log_sigmoid(both[total_heads:] + bias_f)
        level = gate_in + jnp.dot(forget, after, precision=HIGH, preferred_element_type=f32)
        top = jnp.max(level, axis=1, keepdims=True)
        total = jnp.sum(forget, axis=1, keepdims=True)
        part_w = jnp.exp(level - top) * key_scale
        gate_w[0, s * heads : (s + 1) * heads, :span] = jnp.where(
            first, part_w[:heads], part_w[heads : 2 * heads]
        )
        at = spot_lane - s * heads
        packed = packed + jnp.sum(
            jnp.where(local_head & (at == spot_head), total, 0.0)
            + jnp.where(local_head & (at - seqs * heads == spot_head), top, 0.0),
            axis=0,
            keepdims=True,
        )
    stat[me] = jnp.broadcast_to(packed, (8, 128))
    for block in (1, 2, 3):
        start(
            [
                remote(
                    gate_w.at[0],
                    gate_w.at[block],
                    g_recv.at[block],
                    place(0, block // 2, 0, block % 2),
                    core,
                )
            ]
        )
    for off in range(count - 1, 0, -1):
        peer = place(*bits(off))
        start([remote(stat.at[me], stat.at[me], s_recv, peer, core)])
    for c in own_w:
        c.wait()

    def multiply(blocks, slots, s=None):
        low, size = (0, seqs * span) if s is None else (s * span, span)
        pairs = len(slots) // 2

        def choose(i, values):
            out = jnp.int32(values[0])
            for k, v in enumerate(values[1:], 1):
                out = jnp.where(i == k, v, out)
            return out

        def step(i, carry):
            block = choose(i // pairs, blocks) if len(blocks) > 1 else blocks[0]
            at = i % pairs
            out = None
            for off in range(2):
                slot = choose(at, slots[off::2]) if pairs > 1 else slots[off]
                rows = w_rows(slot)
                piece = jnp.dot(
                    xb[block, pl.ds(low, size), rows], wb[rows], preferred_element_type=f32
                )
                out = piece if out is None else out + piece
            acc[block, pl.ds(low, size)] += out
            return carry

        lax.fori_loop(0, len(blocks) * pairs, step, 0)

    for block in range(4):
        acc[block] = jnp.zeros(acc.shape[1:], f32)

    eye = (iota((span, span), 0) == iota((span, span), 1)).astype(f32)
    here = iota((span, seqs * heads), 1)
    chip = iota((count, seqs * heads), 0)
    lane16 = iota((count, seqs * heads), 1)

    def weigh():
        landed(stat.at[pl.ds(0, count - 1)], s_recv)
        table = jnp.concatenate([stat[c, 0:1] for c in range(count)], axis=0)
        beyond = (iota((count, count), 1) > iota((count, count), 0)).astype(f32)
        later = jnp.dot(beyond, table, precision=HIGH, preferred_element_type=f32)
        lift = later[:, : seqs * heads] + table[:, seqs * heads : 2 * seqs * heads]
        highest = jnp.max(lift, axis=0, keepdims=True)
        factor = jnp.exp(lift - highest)
        for block in range(4):
            if block:
                landed(gate_w.at[block], g_recv.at[block])
            turned = lax.dot_general(
                eye,
                gate_w[block][:, :span],
                (((1,), (1,)), ((), ())),
                precision=HIGH,
                preferred_element_type=f32,
            )
            for s in range(seqs):
                column = jnp.sum(
                    jnp.where(here == s * heads + mine, turned, 0.0), axis=1, keepdims=True
                )
                hit = (chip == place(0, block // 2, 0, block % 2)) & (lane16 == s * heads + mine)
                scale = jnp.sum(jnp.where(hit, factor, 0.0), keepdims=True)
                weight[block, s * span : (s + 1) * span] = jnp.broadcast_to(
                    column * scale, (span, 128)
                )
        return highest

    def finish(block, s):
        rows = slice(s * span, (s + 1) * span)
        to = slice(block * span, (block + 1) * span)
        keys = acc[block, rows, :dk].astype(bf16).astype(f32)
        decay[s, to] = (weight[block, rows, 0:1] * keys).astype(bf16)
        vals[s, to] = acc[block, rows, dk:].astype(bf16)

    ones = jnp.ones((8, 4 * span), bf16)
    pick = iota((heads, dk), 0) == mine

    def out_rows(chip):
        return pl.ds(pl.multiple_of(chip * rows_out, rows_out), rows_out)

    def reduce(s):
        d = decay[s]
        sums = lax.dot_general(
            d, vals[s], (((0,), (0,)), ((), ())), preferred_element_type=f32
        )
        high = sums.astype(bf16)
        state[s] = high
        for off in range(count - 1, 0, -1):
            peer = place(*bits(off))
            start(
                [remote(state.at[s, out_rows(peer)], rmem.at[s, me], m_recv.at[s], peer, core)]
            )
        low = (sums - high.astype(f32)).astype(bf16)
        norms = jnp.dot(ones, d, preferred_element_type=f32)
        query = jnp.sum(
            jnp.where(pick, new_query[s].astype(f32), 0.0), axis=0, keepdims=True
        )
        wide = jnp.broadcast_to(query, (8, dk)).astype(bf16)
        seen = jnp.dot(wide, high, preferred_element_type=f32) + jnp.dot(
            wide, low, preferred_element_type=f32
        )
        for k in range(dv // 128):
            aux[s, k : k + 1] = seen[0:1, k * 128 : (k + 1) * 128]
        for k in range(dk // 128):
            aux[s, 4 + k : 5 + k] = norms[0:1, k * 128 : (k + 1) * 128]
        dot_norm = jnp.sum(query * norms[0:1], axis=1, keepdims=True)
        aux[s, 6:8] = jnp.broadcast_to(dot_norm, (2, 128))
        for off in range(count - 1, 0, -1):
            start([remote(aux.at[s], raux.at[s, me], a_recv.at[s], place(*bits(off)), core)])
        rmem[s, me] = state[s, out_rows(me)]
        raux[s, me] = aux[s]

    w_wait(1)
    start(w_relay(1, to_far, 9))
    start(w_relay(1, to_y, 3))
    w_wait(4)
    start(w_relay(4, to_y, 6))
    start(w_relay(4, to_far, 12, inner), inner)
    w_wait(2)
    multiply([0], [0, 2, 1, 4])
    landed(pass_w, w_recv.at[0])
    start([remote(pass_w, wb.at[w_rows(1)], w_recv.at[5], to_z, core)])
    start(tokens[2])
    start([remote(pass_w, wb.at[w_rows(1)], w_recv.at[13], to_mid, core, inner)], inner)
    for unit in range(3, UNITS):
        start(tokens[unit])
    go_w(8)
    w_wait(3)
    multiply([0], [8, 3])
    go_x(1, (0, 1))
    highest = weigh()
    go_w(5)
    start(w_relay(5, to_far, 13, inner), inner)
    w_wait(6)
    go_x(1, (2, 3))
    multiply([0], [5, 6])
    go_w(12)
    w_wait(10)
    go_x(2, (0, 1))
    multiply([0], [12, 10])
    go_x(1, (4, 5))
    go_x(2, (2, 3))
    d_all(1, 0)
    multiply([1], [0, 2, 1, 4, 8, 3, 5, 6, 12, 10], 0)
    go_x(1, (6, 7))
    go_w(9)
    w_wait(7)
    multiply([0], [9, 7])
    go_x(2, (4,))
    d_all(1, 1)
    multiply([1], [0, 2, 1, 4, 8, 3, 5, 6, 12, 10], 1)
    d_all(2, 0)
    go_x(2, (5,))
    multiply([2], [0, 2, 1, 4, 8, 3, 5, 6, 12, 10], 0)
    go_x(3, (0, 1))
    go_x(2, (6,))
    go_w(13)
    w_wait(14)
    go_x(3, (2, 3))
    multiply([0, 1], [13, 14])
    multiply([1], [9, 7])
    go_x(2, (7,))
    d_all(3, 0)
    multiply([3], [0, 2, 1, 4, 8, 3, 5, 6, 12, 10], 0)
    multiply([2, 3], [9, 7, 13, 14], 0)
    go_x(3, (4, 5))
    d_all(2, 1)
    multiply([2], [0, 2, 1, 4, 8, 3, 5, 6, 12, 10, 9, 7, 13, 14], 1)
    w_wait(11)
    w_wait(15)
    go_x(3, (6,))
    multiply([0, 1, 2, 3], [11, 15], 0)
    for block in range(4):
        finish(block, 0)
    reduce(0)
    go_x(3, (7,))
    multiply([0, 1, 2], [11, 15], 1)
    for block in range(3):
        finish(block, 1)
    d_all(3, 1)
    multiply([3], [0, 2, 1, 4, 8, 3, 5, 6, 12, 10, 9, 7, 13, 14, 11, 15], 1)
    finish(3, 1)
    reduce(1)

    def stack(ref):
        return jnp.concatenate([ref[s].astype(f32) for s in range(seqs)], axis=0)

    queries = stack(new_query)
    own = jnp.sum(queries * stack(new_key), axis=1, keepdims=True) * key_scale
    own_head = iota((seqs * heads, heads), 0) % heads == iota((seqs * heads, heads), 1)

    def gate_column(block):
        wide = jnp.concatenate(
            [jnp.broadcast_to(block[s : s + 1], (heads, heads)) for s in range(seqs)], axis=0
        )
        return jnp.sum(jnp.where(own_head, wide, 0.0), axis=1, keepdims=True)

    gate_in, gate_f = gate_column(new_gates[0]), log_sigmoid(gate_column(new_gates[1]))
    token_values = stack(new_value)
    top = upright(highest)
    max_out[...] = top

    read_rows, norm_rows, dot_rows = [], [], []
    for s in range(seqs):
        landed(rmem.at[s, pl.ds(0, count - 1)], m_recv.at[s])
        landed(raux.at[s, pl.ds(0, count - 1)], a_recv.at[s])
        for h in range(heads):
            srcs = [
                (a * 2 + h // 2) * 4 + b * 2 + h % 2 for a in range(2) for b in range(2)
            ]
            mem = rmem[s, srcs[0]].astype(f32)
            both = raux[s, srcs[0]]
            for src in srcs[1:]:
                mem = mem + rmem[s, src].astype(f32)
                both = both + raux[s, src]
            memory_out[s, h] = mem.astype(bf16)
            read_rows.append(
                jnp.concatenate([both[k : k + 1] for k in range(dv // 128)], 1)
            )
            norm_rows.append(
                jnp.concatenate([both[4 + k : 5 + k] for k in range(dk // 128)], 1)
            )
            dot_rows.append(both[6:7, 0:1])
    query_state = jnp.concatenate(read_rows, axis=0)
    norm_all = jnp.concatenate(norm_rows, axis=0)
    query_norm = jnp.concatenate(dot_rows, axis=0)
    take = (
        iota((dk, rows_out), 0) == me * rows_out + iota((dk, rows_out), 1)
    ).astype(f32)
    norm_out[...] = jnp.dot(norm_all, take, precision=HIGH, preferred_element_type=f32)
    mixed = jnp.maximum(gate_f + top, gate_in)
    carried = jnp.exp(gate_f + top - mixed)
    fresh = jnp.exp(gate_in - mixed)
    numer = carried * query_state + (fresh * own) * token_values
    denom = carried * query_norm + fresh * own
    read_out[...] = (numer / jnp.maximum(jnp.abs(denom), 1.0)).astype(bf16)
    for copy, when in sent:
        if when is None:
            copy.wait_send()
        else:
            pl.when(when)(copy.wait_send)


def hand_on(memory, norm, top, read, memory_out, norm_out, max_out, read_out):
    seqs, heads = max_out.shape
    memory_out[...] = memory[...]
    at = lax.broadcasted_iota(jnp.int32, (seqs * heads, heads), 0)
    to = lax.broadcasted_iota(jnp.int32, (seqs * heads, heads), 1)
    wide = read[...].astype(jnp.float32)
    for s in range(seqs):
        rows = slice(s * heads, (s + 1) * heads)
        norm_out[s] = norm[rows]
        read_out[s] = wide[rows].astype(jnp.bfloat16)
        max_out[s : s + 1] = jnp.sum(
            jnp.where(at == s * heads + to, top[...], 0.0), axis=0, keepdims=True
        )


def by_head(
    prompt,
    w_key,
    w_value,
    w_igate,
    w_fgate,
    input_bias,
    forget_bias,
    new_query,
    new_key,
    new_value,
    new_gates,
):
    count = lax.axis_size("sp")
    seqs, span, width = prompt.shape
    depth = w_key.shape[0]
    heads, dk = new_query.shape[1:]
    dv = new_value.shape[2]
    rows = seqs * span
    vmem = pl.BlockSpec(memory_space=pltpu.VMEM)
    hbm = pl.BlockSpec(memory_space=pl.ANY)
    dma = pltpu.SemaphoreType.DMA
    memory, norm, top, read = pl.pallas_call(
        kernel,
        out_shape=(
            jax.ShapeDtypeStruct((seqs, heads, dk // count, dv), jnp.bfloat16),
            jax.ShapeDtypeStruct((seqs * heads, dk // count), jnp.float32),
            jax.ShapeDtypeStruct((seqs * heads, 1), jnp.float32),
            jax.ShapeDtypeStruct((seqs * heads, dv), jnp.bfloat16),
        ),
        in_specs=[hbm, hbm, hbm] + [vmem] * 8,
        out_specs=(vmem, vmem, vmem, vmem),
        scratch_shapes=[
            pltpu.VMEM((4, rows, width), jnp.bfloat16),
            pltpu.VMEM((width, dk + dv), jnp.bfloat16),
            pltpu.VMEM((depth, dk + dv), jnp.bfloat16),
            pltpu.VMEM((4, rows, dk + dv), jnp.float32),
            pltpu.VMEM((seqs, 4 * span, dk), jnp.bfloat16),
            pltpu.VMEM((seqs, 4 * span, dv), jnp.bfloat16),
            pltpu.VMEM((4, rows, 128), jnp.float32),
            pltpu.VMEM((4, 8, 256), jnp.float32),
            pltpu.VMEM((count, 8, 128), jnp.float32),
            pltpu.VMEM((seqs, dk, dv), jnp.bfloat16),
            pltpu.VMEM((seqs, 8, 128), jnp.float32),
            pltpu.VMEM((seqs, count, dk // count, dv), jnp.bfloat16),
            pltpu.VMEM((seqs, count, 8, 128), jnp.float32),
            dma((4,)),
            dma((SENDS,)),
            dma((4, UNITS)),
            dma((4, UNITS)),
            dma((16,)),
            dma((4,)),
            dma,
            dma((seqs,)),
            dma((seqs,)),
        ],
        compiler_params=pltpu.CompilerParams(
            collective_id=0, has_side_effects=True, vmem_limit_bytes=60 * 1024 * 1024
        ),
    )(
        prompt,
        w_key,
        w_value,
        w_igate.T,
        w_fgate.T,
        input_bias[None],
        forget_bias[None],
        new_query,
        new_key,
        new_value,
        new_gates,
    )
    return pl.pallas_call(
        hand_on,
        out_shape=(
            jax.ShapeDtypeStruct((seqs, heads, dk // count, dv), jnp.bfloat16),
            jax.ShapeDtypeStruct((seqs, heads, dk // count), jnp.float32),
            jax.ShapeDtypeStruct((seqs, heads), jnp.float32),
            jax.ShapeDtypeStruct((seqs, heads, dv), jnp.bfloat16),
        ),
        in_specs=[vmem] * 4,
        out_specs=(vmem,) * 4,
    )(memory, norm, top, read)


def chosen(*args):
    prompt, new_query, new_value = args[0], args[7], args[9]
    heads = new_query.shape[1]
    count = lax.axis_size("sp")
    fits = (
        lax.axis_size("tp") == 2
        and heads == 4
        and count == 16
        and prompt.shape[0] == 2
        and new_query.shape[2] == 256
        and new_value.shape[2] == 512
    )
    return by_head(*args) if fits else per_device(*args)


def entering(value, axis, join, neutral):
    count, mine = (lax.axis_size(axis), lax.axis_index(axis))
    pieces = lax.all_gather(value, axis)
    pieces = pieces[::-1]
    mine = count - 1 - mine
    so_far = jnp.full_like(value, 0) + jnp.asarray(neutral, value.dtype)

    def turn(position, so_far):
        longer = join(so_far, pieces[position])
        return jnp.where(position < mine, longer, so_far)

    return lax.fori_loop(0, count - 1, turn, so_far)


def add_pair(earlier, later):
    return earlier + later


def per_device(
    prompt,
    w_key,
    w_value,
    w_igate,
    w_fgate,
    input_bias,
    forget_bias,
    new_query,
    new_key,
    new_value,
    new_gates,
):
    seq_count, span_len, model_width = prompt.shape
    local_heads = new_query.shape[1]
    key_size = new_query.shape[2]
    value_size = new_value.shape[2]
    key_scale = key_size ** (-0.5)
    token_rows = prompt.reshape(seq_count * span_len, model_width)
    whole_key, whole_value = (
        lax.all_gather(w_key, "sp", axis=0, tiled=True),
        lax.all_gather(w_value, "sp", axis=0, tiled=True),
    )
    key_rows = jnp.dot(token_rows, whole_key, preferred_element_type=jnp.float32).astype(
        jnp.bfloat16
    )
    value_rows = jnp.dot(token_rows, whole_value, preferred_element_type=jnp.float32).astype(
        jnp.bfloat16
    )
    head_start = lax.axis_index("tp") * local_heads
    input_all = jnp.dot(token_rows, w_igate, preferred_element_type=jnp.float32) + input_bias
    forget_all = jnp.dot(token_rows, w_fgate, preferred_element_type=jnp.float32) + forget_bias
    input_gate = lax.dynamic_slice_in_dim(input_all, head_start, local_heads, 1).reshape(
        seq_count, span_len, local_heads
    )
    log_forget = jax.nn.log_sigmoid(
        lax.dynamic_slice_in_dim(forget_all, head_start, local_heads, 1)
    ).reshape(seq_count, span_len, local_heads)
    block_total = jnp.sum(log_forget, axis=1)
    forget_after = block_total[:, None] - jnp.cumsum(log_forget, axis=1)
    log_weight = forget_after + input_gate
    block_max = jnp.max(log_weight, axis=1)
    key_blocks = key_rows.reshape(seq_count, span_len, local_heads, key_size).astype(jnp.float32)
    decayed = (jnp.exp(log_weight - block_max[:, None])[..., None] * key_scale * key_blocks).astype(
        jnp.bfloat16
    )
    value_blocks = value_rows.reshape(seq_count, span_len, local_heads, value_size)
    block_norm = jnp.sum(decayed.astype(jnp.float32), axis=1)
    later_total = entering(block_total, "sp", add_pair, jnp.zeros_like(block_total))
    block_lift = later_total + block_max
    global_max = lax.pmax(block_lift, "sp")
    factor = jnp.exp(block_lift - global_max)
    scaled_norm = factor[:, :, None] * block_norm
    query_full = new_query.astype(jnp.float32)
    block_state = jnp.einsum(
        "sthk,sthv->shkv", decayed, value_blocks, preferred_element_type=jnp.float32
    )
    scaled_state = factor[:, :, None, None] * block_state
    memory_rows, norm_rows = (
        lax.psum_scatter(scaled_state, "sp", scatter_dimension=2, tiled=True),
        lax.psum_scatter(scaled_norm, "sp", scatter_dimension=2, tiled=True),
    )
    token_score = jnp.einsum(
        "shk,sthk->sth", new_query, decayed, preferred_element_type=jnp.float32
    )
    score_high = token_score.astype(jnp.bfloat16)
    score_low = (token_score - score_high.astype(jnp.float32)).astype(jnp.bfloat16)
    weighted = jnp.einsum(
        "sth,sthv->shv", score_high, value_blocks, preferred_element_type=jnp.float32
    )
    weighted = weighted + jnp.einsum(
        "sth,sthv->shv", score_low, value_blocks, preferred_element_type=jnp.float32
    )
    partial_state = factor[..., None] * weighted
    partial_norm = jnp.sum(query_full * scaled_norm, axis=-1)
    query_state, query_norm = lax.psum((partial_state, partial_norm), "sp")
    forget_new = jax.nn.log_sigmoid(new_gates[1])
    input_new = new_gates[0]
    mixed = jnp.maximum(forget_new + global_max, input_new)
    carried = jnp.exp(forget_new + global_max - mixed)
    fresh = jnp.exp(input_new - mixed)
    own_score = jnp.sum(query_full * new_key.astype(jnp.float32), axis=-1) * key_scale
    numer = carried[..., None] * query_state + (fresh * own_score)[..., None] * new_value.astype(
        jnp.float32
    )
    denom = carried * query_norm + fresh * own_score
    first_read = (numer / jnp.maximum(jnp.abs(denom), 1.0)[..., None]).astype(jnp.bfloat16)
    return (memory_rows.astype(jnp.bfloat16), norm_rows, global_max, first_read)


def solution(mesh):
    placed = (
        P(None, "sp", None),
        P("sp", "tp"),
        P("sp", "tp"),
        P(),
        P(),
        P(),
        P(),
        P(None, "tp", None),
        P(None, "tp", None),
        P(None, "tp", None),
        P(None, None, "tp"),
    )
    return jax.shard_map(
        chosen,
        mesh=mesh,
        in_specs=placed,
        out_specs=(
            P(None, "tp", "sp", None),
            P(None, "tp", "sp"),
            P(None, "tp"),
            P(None, "tp", None),
        ),
        check_vma=False,
    )
```

```python
import functools
import jax
import jax.numpy as jnp
from jax import lax
from jax.experimental import pallas as pl
from jax.experimental.pallas import tpu as pltpu
from jax.sharding import PartitionSpec as P

HIGH = lax.Precision.HIGHEST
PARTS = 4
KINDS = ("x1", "x2", "x3", "xa", "ya", "xb", "yb", "xc", "yc")
SENDS = 180
SCHEDULE = (
    ("far",),
    ("px2",),
    ("tx", 0),
    ("mid",),
    ("tz", 0),
    ("near",),
    ("px",),
    ("tx", 1),
    ("yown",),
    ("x2", 0),
    ("tx", 2),
    ("w", 8),
    ("tb", 0),
    ("tx", 3),
    ("tz", 1),
    ("p",),
    ("w", 4),
    ("w", 1),
    ("tz", 2),
    ("pm",),
    ("tx", 4),
    ("w", 12),
    ("tx", 5),
    ("x1", 0),
    ("x1", 1),
    ("x2", 1),
    ("tx", 6),
    ("tz", 3),
    ("w", 2),
    ("w", 5),
    ("x1", 2),
    ("xb", 0),
    ("x3", 0),
    ("x1", 3),
    ("gates",),
    ("w", 3),
    ("x1", 4),
    ("x1", 5),
    ("ta", 0),
    ("tb", 1),
    ("ta", 1),
    ("tx", 7),
    ("x1", 6),
    ("mm", 0, 2, (8, 4, 1, 12)),
    ("x2", 2),
    ("w", 10),
    ("x3", 1),
    ("mm", 0, 2, (2, 5, 0, 3)),
    ("ta", 2),
    ("yb", 0),
    ("w", 9),
    ("x1", 7),
    ("x2", 3),
    ("d", "x1", 0),
    ("d", "x1", 4),
    ("mm", 2, 2, (8, 4, 1, 12)),
    ("yb", 1),
    ("w", 6),
    ("mm", 2, 2, (2, 5, 0, 3)),
    ("xc", 0),
    ("w", 14),
    ("tell_all",),
    ("x3", 2),
    ("ta", 3),
    ("w", 13),
    ("tb", 2),
    ("xa", 0),
    ("xa", 1),
    ("x3", 3),
    ("tb", 3),
    ("d", "x2", 0),
    ("d", "x3", 0),
    ("mm", 4, 2, (8, 4, 1, 12)),
    ("mm", 2, 2, (10, 9, 6, 14)),
    ("mm", 4, 2, (2, 5, 0, 3)),
    ("xa", 2),
    ("mm", 0, 2, (10, 9, 6, 14)),
    ("yb", 2),
    ("yc", 0),
    ("yb", 3),
    ("mm", 4, 2, (10, 9, 6, 14)),
    ("xc", 1),
    ("w", 7),
    ("xc", 2),
    ("ya", 0),
    ("xa", 3),
    ("weigh",),
    ("xc", 3),
    ("ya", 1),
    ("w", 11),
    ("xb", 1),
    ("w", 15),
    ("mm", 4, 2, (13, 7, 11, 15)),
    ("mm", 0, 2, (13, 7, 11, 15)),
    ("mm", 2, 2, (13, 7, 11, 15)),
    ("finish", 0, 2, 4, 5),
    ("reduce", 0),
    ("d1", "xa", 0),
    ("d1", "ya", 0),
    ("mma", 6, 1, 0),
    ("d1", "xb", 0),
    ("d1", "yb", 0),
    ("d1", "xc", 0),
    ("d1", "yc", 0),
    ("mma", 7, 2, 0),
    ("yc", 1),
    ("d1", "xa", 1),
    ("d1", "ya", 1),
    ("mma", 6, 1, 1),
    ("d1", "xb", 1),
    ("d1", "yb", 1),
    ("d1", "xc", 1),
    ("d1", "yc", 1),
    ("mma", 7, 2, 1),
    ("ya", 2),
    ("yc", 2),
    ("xb", 2),
    ("ya", 3),
    ("xb", 3),
    ("yc", 3),
    ("d1", "xa", 2),
    ("d1", "ya", 2),
    ("mma", 6, 1, 2),
    ("d1", "xb", 2),
    ("d1", "yb", 2),
    ("d1", "xc", 2),
    ("d1", "yc", 2),
    ("mma", 7, 2, 2),
    ("finish", 1, 3),
    ("d1", "xa", 3),
    ("d1", "ya", 3),
    ("mma", 6, 1, 3),
    ("d1", "xb", 3),
    ("d1", "yb", 3),
    ("d1", "xc", 3),
    ("d1", "yc", 3),
    ("mma", 7, 2, 3),
    ("reduce_on",),
    ("finish", 6, 7, 8),
    ("reduce", 1),
)


def flip(bit, change):
    return bit + change - 2 * bit * change


def log_sigmoid(v):
    return jnp.minimum(v, 0.0) - jnp.log1p(jnp.exp(-jnp.abs(v)))


def iota(shape, dim):
    return lax.broadcasted_iota(jnp.int32, shape, dim)


def kernel(
    prompt,
    w_key,
    w_value,
    w_igate,
    w_fgate,
    input_bias,
    forget_bias,
    new_query,
    new_key,
    new_value,
    new_gates,
    memory_out,
    norm_out,
    max_out,
    read_out,
    xb,
    wb,
    pass_w,
    acc,
    decay,
    vals,
    weight,
    gate_w,
    stat,
    state,
    late_state,
    pair_state,
    y_in,
    aux,
    pair_aux,
    y_aux,
    rmem,
    raux,
    local_sem,
    ready,
    sends,
    x_recv,
    d_recv,
    w_recv,
    g_recv,
    s_recv,
    y_recv,
    m_recv,
    a_recv,
):
    count = lax.axis_size("sp")
    me = lax.axis_index("sp")
    core = lax.axis_index("tp")
    seqs, span, width = prompt.shape
    depth = w_key.shape[0]
    heads = new_query.shape[1]
    dk = new_query.shape[2]
    dv = new_value.shape[2]
    total_heads = input_bias.shape[1]
    key_scale = dk ** (-0.5)
    cut = width // (2 * PARTS)
    half = span // 2
    rows_out = dk // count
    zh, zl, y, x = me // 8, (me // 4) % 2, (me // 2) % 2, me % 2
    mine = zl * 2 + x
    inner = zh != zl
    outer = zh == zl
    bf16, f32 = jnp.bfloat16, jnp.float32

    def place(dh, dl, dy, dx):
        return flip(zh, dh) * 8 + flip(zl, dl) * 4 + flip(y, dy) * 2 + flip(x, dx)

    sent = []

    def remote(src, dst, recv, sp, tp, when=None):
        copy = pltpu.make_async_remote_copy(
            src_ref=src,
            dst_ref=dst,
            send_sem=sends.at[len(sent)],
            recv_sem=recv,
            device_id=(sp, tp),
            device_id_type=pl.DeviceIdType.MESH,
        )
        sent.append((copy, when))
        return copy

    def start(copies, when=None):
        def run():
            for copy in copies:
                copy.start()

        if when is None:
            run()
        else:
            pl.when(when)(run)

    def landed(ref, sem):
        pltpu.make_async_copy(ref, ref, sem).wait()

    to_x, to_y, to_z = place(0, 0, 0, 1), place(0, 0, 1, 0), place(0, 1, 0, 0)
    to_far, to_mid = place(1, 0, 0, 0), place(1, 1, 0, 0)
    barrier = pltpu.get_barrier_semaphore()

    def tell(sem, sp, tp):
        pl.semaphore_signal(
            sem, inc=1, device_id=(sp, tp), device_id_type=pl.DeviceIdType.MESH
        )

    gate_w[...] = jnp.zeros(gate_w.shape, f32)
    for peer in (to_x, to_y, to_z):
        tell(barrier, peer, core)
    tell(barrier, me, 1 - core)

    @pl.when(inner)
    def _():
        tell(barrier, to_mid, core)

    def bits(slot):
        return slot // 8, (slot // 4) % 2, (slot // 2) % 2, slot % 2

    def w_rows(slot):
        return pl.ds(pl.multiple_of(place(*bits(slot)) * depth, depth), depth)

    def group_cols(dl, dx):
        group = flip(zl, dl) * 2 + flip(x, dx)
        kc = pl.ds(pl.multiple_of(group * dk, dk), dk)
        vc = pl.ds(pl.multiple_of(group * dv, dv), dv)
        return kc, vc

    own_x = []
    for s in range(seqs):
        c = pltpu.make_async_copy(
            prompt.at[s], xb.at[pl.ds(s * span, span)], local_sem.at[s]
        )
        c.start()
        own_x.append(c)
    kc, vc = group_cols(0, 0)
    own_w = [
        pltpu.make_async_copy(w_key.at[:, kc], wb.at[w_rows(0), :dk], local_sem.at[2]),
        pltpu.make_async_copy(w_value.at[:, vc], wb.at[w_rows(0), dk:], local_sem.at[3]),
    ]
    for c in own_w:
        c.start()
    pl.semaphore_wait(barrier, 4 + jnp.where(inner, 1, 0))

    def w_own(dl, dx, peer, slot, when=None):
        kc, vc = group_cols(dl, dx)
        rows = w_rows(0)
        return [
            remote(w_key.at[:, kc], wb.at[rows, :dk], w_recv.at[slot], peer, core, when),
            remote(w_value.at[:, vc], wb.at[rows, dk:], w_recv.at[slot], peer, core, when),
        ]

    def w_relay(slot, peer, there, when=None):
        rows = w_rows(slot)
        return [remote(wb.at[rows], wb.at[rows], w_recv.at[there], peer, core, when)]

    def w_wait(slot):
        landed(wb.at[w_rows(slot)], w_recv.at[slot])

    def columns(owner, k):
        return pl.ds(pl.multiple_of((owner * PARTS + k) * cut, cut), cut)

    def rows_of(kind, unit):
        if kind in ("x1", "x2", "x3"):
            chunk = {"x1": 2 + unit // PARTS, "x2": 4, "x3": 5}[kind]
            return chunk * span, span
        chunk = {"a": 6, "b": 7, "c": 8}[kind[1]]
        return chunk * span + (half if kind[0] == "y" else 0), half

    def part(kind, unit, owner):
        low, size = rows_of(kind, unit)
        return xb.at[pl.ds(low, size), columns(owner, unit % PARTS)]

    def sem(table, kind, unit):
        return table.at[KINDS.index(kind), unit]

    def x_own(s, low, size, kind, unit, peer, when=None):
        src = prompt.at[s, pl.ds(low, size), columns(core, unit % PARTS)]
        copy = remote(src, part(kind, unit, core), sem(x_recv, kind, unit), peer, core, when)
        start([copy], when)

    def x_pass(kind, there, unit, peer, when=None):
        copy = remote(
            part(kind, unit, core),
            part(there, unit, core),
            sem(x_recv, there, unit),
            peer,
            core,
            when,
        )
        start([copy], when)

    def only(kind):
        return inner if kind[1] in "bc" else None

    def x_across(kind, unit):
        own = part(kind, unit, core)
        when = only(kind)
        start([remote(own, own, sem(d_recv, kind, unit), me, 1 - core, when)], when)

    def maybe(when, run):
        if when is None:
            run()
        else:
            pl.when(when)(run)

    def x_wait(kind, unit):
        maybe(
            only(kind),
            lambda: landed(part(kind, unit, core), sem(x_recv, kind, unit)),
        )

    def d_wait(kind, unit):
        maybe(
            only(kind),
            lambda: landed(part(kind, unit, 1 - core), sem(d_recv, kind, unit)),
        )

    def go_x(kind, unit):
        x_wait(kind, unit)
        if kind == "x2":
            x_pass("x2", "x3", unit, to_x)
        if kind == "xa":
            x_pass("xa", "ya", unit, to_x)
        if kind == "xc":
            x_pass("xc", "yc", unit, to_x, inner)
        if kind == "x1" and unit >= PARTS:
            k = unit - PARTS
            src = xb.at[pl.ds(3 * span + half, half), columns(core, k)]
            dst = part("yb", k, core)
            start([remote(src, dst, sem(x_recv, "yb", k), to_z, core, outer)], outer)
        x_across(kind, unit)

    def go_w(slot):
        w_wait(slot)
        start(w_relay(slot, to_y, slot + 2))

    first = core == 0

    near, far, mid = (
        w_own(1, 0, to_z, 4),
        w_own(0, 0, to_far, 8),
        w_own(1, 0, to_mid, 12, inner),
    )
    px, y_own = w_own(0, 1, to_x, 1), w_own(0, 0, to_y, 2)
    kc, vc = group_cols(1, 1)
    px2 = [
        remote(w_key.at[:, kc], pass_w.at[:, :dk], w_recv.at[0], to_x, core),
        remote(w_value.at[:, vc], pass_w.at[:, dk:], w_recv.at[0], to_x, core),
    ]

    def greet():
        @pl.when(inner)
        def _():
            tell(ready, to_z, core)
            tell(ready, to_mid, core)

        pl.semaphore_wait(ready, 1)

    w_gate = jnp.concatenate([w_igate[...], w_fgate[...]], axis=0)
    square = iota((total_heads, total_heads), 0) == iota((total_heads, total_heads), 1)

    def upright(row):
        return jnp.sum(jnp.where(square, row, 0.0), axis=1, keepdims=True)

    bias_in, bias_f = upright(input_bias[...]), upright(forget_bias[...])
    after = (iota((span, span), 0) > iota((span, span), 1)).astype(f32)
    spot_head = iota((total_heads, 128), 0) - core * heads
    spot_lane = iota((total_heads, 128), 1)
    local_head = (spot_head >= 0) & (spot_head < heads)
    def gates():
        for c in own_x:
            c.wait()
        packed = jnp.zeros((1, 128), f32)
        for s in range(seqs):
            both = lax.dot_general(
                w_gate,
                xb[s * span : (s + 1) * span],
                (((1,), (1,)), ((), ())),
                preferred_element_type=f32,
            )
            gate_in = both[:total_heads] + bias_in
            forget = log_sigmoid(both[total_heads:] + bias_f)
            level = gate_in + jnp.dot(forget, after, precision=HIGH, preferred_element_type=f32)
            top = jnp.max(level, axis=1, keepdims=True)
            total = jnp.sum(forget, axis=1, keepdims=True)
            part_w = jnp.exp(level - top) * key_scale
            gate_w[0, s * heads : (s + 1) * heads, :span] = jnp.where(
                first, part_w[:heads], part_w[heads : 2 * heads]
            )
            at = spot_lane - s * heads
            packed = packed + jnp.sum(
                jnp.where(local_head & (at == spot_head), total, 0.0)
                + jnp.where(local_head & (at - seqs * heads == spot_head), top, 0.0),
                axis=0,
                keepdims=True,
            )
        stat[me] = jnp.broadcast_to(packed, (8, 128))
        for c in own_w:
            c.wait()

    def tell_all():
        for off in range(count - 1, 0, -1):
            peer = place(*bits(off))
            start([remote(stat.at[me], stat.at[me], s_recv, peer, core)])
        for block, peer in ((1, to_x), (2, to_z), (3, place(0, 1, 0, 1))):
            start([remote(gate_w.at[0], gate_w.at[block], g_recv.at[block], peer, core)])
        for block, peer in ((4, to_mid), (5, place(1, 1, 0, 1))):
            copy = remote(
                gate_w.at[0], gate_w.at[block], g_recv.at[block], peer, core, inner
            )
            start([copy], inner)

    def choose(i, values):
        out = jnp.int32(values[0])
        for k, v in enumerate(values[1:], 1):
            out = jnp.where(i == k, v, out)
        return out

    def multiply(low, size, slots):
        width_in = 4 if len(slots) % 4 == 0 else 2

        def step(i, carry):
            out = None
            for off in range(width_in):
                rows = w_rows(choose(i, slots[off::width_in]))
                piece = jnp.dot(
                    xb[pl.ds(low, size), rows], wb[rows], preferred_element_type=f32
                )
                out = piece if out is None else out + piece
            acc[pl.ds(low, size)] += out
            return carry

        lax.fori_loop(0, len(slots) // width_in, step, 0)

    def multiply_part(low, size, k):
        out = None
        for owner in range(2):
            cols = slice((owner * PARTS + k) * cut, (owner * PARTS + k + 1) * cut)
            piece = jnp.dot(xb[low : low + size, cols], wb[cols], preferred_element_type=f32)
            out = piece if out is None else out + piece
        acc[low : low + size] += out

    def zero(i, carry):
        acc[pl.ds(pl.multiple_of(i * span, span), span)] = jnp.zeros((span, dk + dv), f32)
        return carry

    lax.fori_loop(0, 9, zero, 0)

    eye = (iota((span, span), 0) == iota((span, span), 1)).astype(f32)
    here = iota((span, seqs * heads), 1)
    chip = iota((count, seqs * heads), 0)
    lane16 = iota((count, seqs * heads), 1)

    def weigh():
        landed(stat.at[pl.ds(0, count - 1)], s_recv)
        table = jnp.concatenate([stat[c, 0:1] for c in range(count)], axis=0)
        beyond = (iota((count, count), 1) > iota((count, count), 0)).astype(f32)
        later = jnp.dot(beyond, table, precision=HIGH, preferred_element_type=f32)
        lift = later[:, : seqs * heads] + table[:, seqs * heads : 2 * seqs * heads]
        highest = jnp.max(lift, axis=0, keepdims=True)
        factor = jnp.exp(lift - highest)
        weight[8 * span : 9 * span] = jnp.zeros((span, 128), f32)

        def column(block, s):
            turned = lax.dot_general(
                eye,
                gate_w[block][:, :span],
                (((1,), (1,)), ((), ())),
                precision=HIGH,
                preferred_element_type=f32,
            )
            dh, pos = (0, block) if block < 4 else (1, 2 + block % 2)
            lane = s * heads + mine
            hit = (chip == place(dh, pos // 2, 0, pos % 2)) & (lane16 == lane)
            scale = jnp.sum(jnp.where(hit, factor, 0.0), keepdims=True)
            one = jnp.sum(jnp.where(here == lane, turned, 0.0), axis=1, keepdims=True)
            return jnp.broadcast_to(one * scale, (span, 128))

        for block in range(4):
            if block:
                landed(gate_w.at[block], g_recv.at[block])
            weight[pl.ds((2 * block if block < 2 else 2 + block) * span, span)] = column(block, 0)
            late = column(block, 1)
            if block < 2:
                weight[pl.ds((2 * block + 1) * span, span)] = late
            else:
                for chunk in (6, 7):
                    low = chunk * span + (block - 2) * half
                    weight[pl.ds(low, half)] = late[(chunk - 6) * half : (chunk - 5) * half]

        @pl.when(inner)
        def _():
            for block in (4, 5):
                landed(gate_w.at[block], g_recv.at[block])
                low = 8 * span + (block - 4) * half
                weight[pl.ds(low, half)] = column(block, 1)[half:]

        return highest

    to_chunk = (0, 4, 1, 5, 2, 3, 6, 7, 8)

    def finish(chunk):
        rows = slice(chunk * span, (chunk + 1) * span)
        to = slice(to_chunk[chunk] * span, (to_chunk[chunk] + 1) * span)
        keys = acc[rows, :dk].astype(bf16).astype(f32)
        decay[to] = (weight[rows, 0:1] * keys).astype(bf16)
        vals[to] = acc[rows, dk:].astype(bf16)

    pick = iota((heads, dk), 0) == mine

    def out_rows(chip):
        return pl.ds(pl.multiple_of(chip * rows_out, rows_out), rows_out)

    def reduce(s):
        span_rows = slice(0, 4 * span) if s == 0 else slice(4 * span, 9 * span)
        d = decay[span_rows]
        ones = jnp.ones((8, d.shape[0]), bf16)
        sums = lax.dot_general(
            d, vals[span_rows], (((0,), (0,)), ((), ())), preferred_element_type=f32
        )
        high = sums.astype(bf16)
        if s == 0:
            for block in range(count // 2):
                low = (block // 2) * 2 * rows_out
                state[block % 2, low : low + 2 * rows_out] = high[
                    block * 2 * rows_out : (block + 1) * 2 * rows_out
                ]
            start([remote(state.at[1 - y], y_in, y_recv.at[0], to_y, core)])
        else:
            late_state[...] = high
            for off in range(count - 1, 0, -1):
                peer = place(*bits(off))
                src = late_state.at[out_rows(peer)]
                start([remote(src, rmem.at[1, me], m_recv.at[1], peer, core)])
        low = (sums - high.astype(f32)).astype(bf16)
        norms = jnp.dot(ones, d, preferred_element_type=f32)
        query = jnp.sum(
            jnp.where(pick, new_query[s].astype(f32), 0.0), axis=0, keepdims=True
        )
        wide = jnp.broadcast_to(query, (8, dk)).astype(bf16)
        seen = jnp.dot(wide, high, preferred_element_type=f32) + jnp.dot(
            wide, low, preferred_element_type=f32
        )
        for k in range(dv // 128):
            aux[s, k : k + 1] = seen[0:1, k * 128 : (k + 1) * 128]
        for k in range(dk // 128):
            aux[s, 4 + k : 5 + k] = norms[0:1, k * 128 : (k + 1) * 128]
        dot_norm = jnp.sum(query * norms[0:1], axis=1, keepdims=True)
        aux[s, 6:8] = jnp.broadcast_to(dot_norm, (2, 128))
        if s == 0:
            start([remote(aux.at[0], y_aux, y_recv.at[1], to_y, core)])
        else:
            for off in range(count - 1, 0, -1):
                peer = place(*bits(off))
                start([remote(aux.at[1], raux.at[1, me], a_recv.at[1], peer, core)])
            rmem[1, me] = late_state[out_rows(me)]
            raux[1, me] = aux[1]

    spot8 = (zh * 2 + zl) * 2 + x

    def reduce_on():
        landed(y_in, y_recv.at[0])
        pair_state[...] = (state[y].astype(f32) + y_in[...].astype(f32)).astype(bf16)
        landed(y_aux, y_recv.at[1])
        pair_aux[...] = aux[0] + y_aux[...]
        for off in range(count // 2 - 1, 0, -1):
            dh, dl, dx = off // 4, (off // 2) % 2, off % 2
            peer = place(dh, dl, 0, dx)
            spot = (flip(zh, dh) * 2 + flip(zl, dl)) * 2 + flip(x, dx)
            src = pair_state.at[out_rows(spot)]
            start([remote(src, rmem.at[0, spot8], m_recv.at[0], peer, core)])
            start([remote(pair_aux, raux.at[0, spot8], a_recv.at[0], peer, core)])
        rmem[0, spot8] = pair_state[out_rows(spot8)]
        raux[0, spot8] = pair_aux[...]

    streams = {"px": px, "px2": px2, "yown": y_own, "near": near}
    highest = None
    for name, *arg in SCHEDULE:
        if name in streams:
            start(streams[name])
        elif name == "far":
            greet()
            start(far)
        elif name == "mid":
            start(mid, inner)
        elif name == "gates":
            gates()
        elif name == "tell_all":
            tell_all()
        elif name == "tx":
            x_own(arg[0] // PARTS, 0, span, "x1", arg[0], to_x)
        elif name == "tz":
            x_own(0, 0, span, "x2", arg[0], to_z)
        elif name == "ta":
            x_own(1, 0, half, "xa", arg[0], to_z)
        elif name == "tb":
            x_own(1, half, half, "xb", arg[0], to_z, outer)
            x_own(1, half, half, "xc", arg[0], to_mid, inner)
        elif name == "w":
            slot = arg[0]
            w_wait(slot)
            if slot == 1:
                start(w_relay(1, to_far, 9))
            if slot % 4 < 2:
                start(w_relay(slot, to_y, slot + 2))
            if slot in (4, 5):
                start(w_relay(slot, to_far, slot + 8, inner), inner)
        elif name == "p":
            landed(pass_w, w_recv.at[0])
            start([remote(pass_w, wb.at[w_rows(1)], w_recv.at[5], to_z, core)])
        elif name == "pm":
            copy = remote(pass_w, wb.at[w_rows(1)], w_recv.at[13], to_mid, core, inner)
            start([copy], inner)
        elif name in KINDS:
            go_x(name, arg[0])
        elif name == "d":
            kind, low = arg
            for unit in range(low, low + PARTS):
                d_wait(kind, unit)
        elif name == "mm":
            low, chunks, slots = arg
            maybe(
                inner if low >= 7 else None,
                lambda: multiply(low * span, chunks * span, slots),
            )
        elif name == "d1":
            d_wait(*arg)
        elif name == "mma":
            low, chunks, k = arg
            maybe(
                inner if low >= 7 else None,
                lambda: multiply_part(low * span, chunks * span, k),
            )
        elif name == "weigh":
            highest = weigh()
        elif name == "finish":
            for chunk in arg:
                finish(chunk)
        elif name == "reduce":
            reduce(arg[0])
        elif name == "reduce_on":
            reduce_on()

    def stack(ref):
        return jnp.concatenate([ref[s].astype(f32) for s in range(seqs)], axis=0)

    queries = stack(new_query)
    own = jnp.sum(queries * stack(new_key), axis=1, keepdims=True) * key_scale
    own_head = iota((seqs * heads, heads), 0) % heads == iota((seqs * heads, heads), 1)

    def gate_column(block):
        wide = jnp.concatenate(
            [jnp.broadcast_to(block[s : s + 1], (heads, heads)) for s in range(seqs)], axis=0
        )
        return jnp.sum(jnp.where(own_head, wide, 0.0), axis=1, keepdims=True)

    gate_in, gate_f = gate_column(new_gates[0]), log_sigmoid(gate_column(new_gates[1]))
    token_values = stack(new_value)
    top = upright(highest)
    max_out[...] = top

    read_rows, norm_rows, dot_rows = [], [], []
    for s in range(seqs):
        peers = count // 2 - 1 if s == 0 else count - 1
        landed(rmem.at[s, pl.ds(0, peers)], m_recv.at[s])
        landed(raux.at[s, pl.ds(0, peers)], a_recv.at[s])
        for h in range(heads):
            if s == 0:
                srcs = [(a * 2 + h // 2) * 2 + h % 2 for a in range(2)]
            else:
                srcs = [
                    (a * 2 + h // 2) * 4 + b * 2 + h % 2 for a in range(2) for b in range(2)
                ]
            mem = rmem[s, srcs[0]].astype(f32)
            both = raux[s, srcs[0]]
            for src in srcs[1:]:
                mem = mem + rmem[s, src].astype(f32)
                both = both + raux[s, src]
            memory_out[s, h] = mem.astype(bf16)
            read_rows.append(
                jnp.concatenate([both[k : k + 1] for k in range(dv // 128)], 1)
            )
            norm_rows.append(
                jnp.concatenate([both[4 + k : 5 + k] for k in range(dk // 128)], 1)
            )
            dot_rows.append(both[6:7, 0:1])
    query_state = jnp.concatenate(read_rows, axis=0)
    norm_all = jnp.concatenate(norm_rows, axis=0)
    query_norm = jnp.concatenate(dot_rows, axis=0)
    take = (
        iota((dk, rows_out), 0) == me * rows_out + iota((dk, rows_out), 1)
    ).astype(f32)
    norm_out[...] = jnp.dot(norm_all, take, precision=HIGH, preferred_element_type=f32)
    mixed = jnp.maximum(gate_f + top, gate_in)
    carried = jnp.exp(gate_f + top - mixed)
    fresh = jnp.exp(gate_in - mixed)
    numer = carried * query_state + (fresh * own) * token_values
    denom = carried * query_norm + fresh * own
    read_out[...] = (numer / jnp.maximum(jnp.abs(denom), 1.0)).astype(bf16)
    for copy, when in sent:
        if when is None:
            copy.wait_send()
        else:
            pl.when(when)(copy.wait_send)


def hand_on(memory, norm, top, read, memory_out, norm_out, max_out, read_out):
    seqs, heads = max_out.shape
    memory_out[...] = memory[...]
    at = lax.broadcasted_iota(jnp.int32, (seqs * heads, heads), 0)
    to = lax.broadcasted_iota(jnp.int32, (seqs * heads, heads), 1)
    wide = read[...].astype(jnp.float32)
    for s in range(seqs):
        rows = slice(s * heads, (s + 1) * heads)
        norm_out[s] = norm[rows]
        read_out[s] = wide[rows].astype(jnp.bfloat16)
        max_out[s : s + 1] = jnp.sum(
            jnp.where(at == s * heads + to, top[...], 0.0), axis=0, keepdims=True
        )


def by_head(
    prompt,
    w_key,
    w_value,
    w_igate,
    w_fgate,
    input_bias,
    forget_bias,
    new_query,
    new_key,
    new_value,
    new_gates,
):
    count = lax.axis_size("sp")
    seqs, span, width = prompt.shape
    depth = w_key.shape[0]
    heads, dk = new_query.shape[1:]
    dv = new_value.shape[2]
    rows = seqs * span
    vmem = pl.BlockSpec(memory_space=pltpu.VMEM)
    hbm = pl.BlockSpec(memory_space=pl.ANY)
    dma = pltpu.SemaphoreType.DMA
    memory, norm, top, read = pl.pallas_call(
        kernel,
        out_shape=(
            jax.ShapeDtypeStruct((seqs, heads, dk // count, dv), jnp.bfloat16),
            jax.ShapeDtypeStruct((seqs * heads, dk // count), jnp.float32),
            jax.ShapeDtypeStruct((seqs * heads, 1), jnp.float32),
            jax.ShapeDtypeStruct((seqs * heads, dv), jnp.bfloat16),
        ),
        in_specs=[hbm, hbm, hbm] + [vmem] * 8,
        out_specs=(vmem, vmem, vmem, vmem),
        scratch_shapes=[
            pltpu.VMEM((9 * span, width), jnp.bfloat16),
            pltpu.VMEM((width, dk + dv), jnp.bfloat16),
            pltpu.VMEM((depth, dk + dv), jnp.bfloat16),
            pltpu.VMEM((9 * span, dk + dv), jnp.float32),
            pltpu.VMEM((9 * span, dk), jnp.bfloat16),
            pltpu.VMEM((9 * span, dv), jnp.bfloat16),
            pltpu.VMEM((9 * span, 128), jnp.float32),
            pltpu.VMEM((6, 8, 256), jnp.float32),
            pltpu.VMEM((count, 8, 128), jnp.float32),
            pltpu.VMEM((2, dk // 2, dv), jnp.bfloat16),
            pltpu.VMEM((dk, dv), jnp.bfloat16),
            pltpu.VMEM((dk // 2, dv), jnp.bfloat16),
            pltpu.VMEM((dk // 2, dv), jnp.bfloat16),
            pltpu.VMEM((seqs, 8, 128), jnp.float32),
            pltpu.VMEM((8, 128), jnp.float32),
            pltpu.VMEM((8, 128), jnp.float32),
            pltpu.VMEM((seqs, count, dk // count, dv), jnp.bfloat16),
            pltpu.VMEM((seqs, count, 8, 128), jnp.float32),
            dma((4,)),
            pltpu.SemaphoreType.REGULAR,
            dma((SENDS,)),
            dma((len(KINDS), 2 * PARTS)),
            dma((len(KINDS), 2 * PARTS)),
            dma((16,)),
            dma((6,)),
            dma,
            dma((2,)),
            dma((seqs,)),
            dma((seqs,)),
        ],
        compiler_params=pltpu.CompilerParams(
            collective_id=0, has_side_effects=True, vmem_limit_bytes=60 * 1024 * 1024
        ),
    )(
        prompt,
        w_key,
        w_value,
        w_igate.T,
        w_fgate.T,
        input_bias[None],
        forget_bias[None],
        new_query,
        new_key,
        new_value,
        new_gates,
    )
    return pl.pallas_call(
        hand_on,
        out_shape=(
            jax.ShapeDtypeStruct((seqs, heads, dk // count, dv), jnp.bfloat16),
            jax.ShapeDtypeStruct((seqs, heads, dk // count), jnp.float32),
            jax.ShapeDtypeStruct((seqs, heads), jnp.float32),
            jax.ShapeDtypeStruct((seqs, heads, dv), jnp.bfloat16),
        ),
        in_specs=[vmem] * 4,
        out_specs=(vmem,) * 4,
    )(memory, norm, top, read)


def chosen(*args):
    prompt, new_query, new_value = args[0], args[7], args[9]
    heads = new_query.shape[1]
    count = lax.axis_size("sp")
    fits = (
        lax.axis_size("tp") == 2
        and heads == 4
        and count == 16
        and prompt.shape[0] == 2
        and new_query.shape[2] == 256
        and new_value.shape[2] == 512
    )
    return by_head(*args) if fits else per_device(*args)


def entering(value, axis, join, neutral):
    count, mine = (lax.axis_size(axis), lax.axis_index(axis))
    pieces = lax.all_gather(value, axis)
    pieces = pieces[::-1]
    mine = count - 1 - mine
    so_far = jnp.full_like(value, 0) + jnp.asarray(neutral, value.dtype)

    def turn(position, so_far):
        longer = join(so_far, pieces[position])
        return jnp.where(position < mine, longer, so_far)

    return lax.fori_loop(0, count - 1, turn, so_far)


def add_pair(earlier, later):
    return earlier + later


def per_device(
    prompt,
    w_key,
    w_value,
    w_igate,
    w_fgate,
    input_bias,
    forget_bias,
    new_query,
    new_key,
    new_value,
    new_gates,
):
    seq_count, span_len, model_width = prompt.shape
    local_heads = new_query.shape[1]
    key_size = new_query.shape[2]
    value_size = new_value.shape[2]
    key_scale = key_size ** (-0.5)
    token_rows = prompt.reshape(seq_count * span_len, model_width)
    whole_key, whole_value = (
        lax.all_gather(w_key, "sp", axis=0, tiled=True),
        lax.all_gather(w_value, "sp", axis=0, tiled=True),
    )
    key_rows = jnp.dot(token_rows, whole_key, preferred_element_type=jnp.float32).astype(
        jnp.bfloat16
    )
    value_rows = jnp.dot(token_rows, whole_value, preferred_element_type=jnp.float32).astype(
        jnp.bfloat16
    )
    head_start = lax.axis_index("tp") * local_heads
    input_all = jnp.dot(token_rows, w_igate, preferred_element_type=jnp.float32) + input_bias
    forget_all = jnp.dot(token_rows, w_fgate, preferred_element_type=jnp.float32) + forget_bias
    input_gate = lax.dynamic_slice_in_dim(input_all, head_start, local_heads, 1).reshape(
        seq_count, span_len, local_heads
    )
    log_forget = jax.nn.log_sigmoid(
        lax.dynamic_slice_in_dim(forget_all, head_start, local_heads, 1)
    ).reshape(seq_count, span_len, local_heads)
    block_total = jnp.sum(log_forget, axis=1)
    forget_after = block_total[:, None] - jnp.cumsum(log_forget, axis=1)
    log_weight = forget_after + input_gate
    block_max = jnp.max(log_weight, axis=1)
    key_blocks = key_rows.reshape(seq_count, span_len, local_heads, key_size).astype(jnp.float32)
    decayed = (jnp.exp(log_weight - block_max[:, None])[..., None] * key_scale * key_blocks).astype(
        jnp.bfloat16
    )
    value_blocks = value_rows.reshape(seq_count, span_len, local_heads, value_size)
    block_norm = jnp.sum(decayed.astype(jnp.float32), axis=1)
    later_total = entering(block_total, "sp", add_pair, jnp.zeros_like(block_total))
    block_lift = later_total + block_max
    global_max = lax.pmax(block_lift, "sp")
    factor = jnp.exp(block_lift - global_max)
    scaled_norm = factor[:, :, None] * block_norm
    query_full = new_query.astype(jnp.float32)
    block_state = jnp.einsum(
        "sthk,sthv->shkv", decayed, value_blocks, preferred_element_type=jnp.float32
    )
    scaled_state = factor[:, :, None, None] * block_state
    memory_rows, norm_rows = (
        lax.psum_scatter(scaled_state, "sp", scatter_dimension=2, tiled=True),
        lax.psum_scatter(scaled_norm, "sp", scatter_dimension=2, tiled=True),
    )
    token_score = jnp.einsum(
        "shk,sthk->sth", new_query, decayed, preferred_element_type=jnp.float32
    )
    score_high = token_score.astype(jnp.bfloat16)
    score_low = (token_score - score_high.astype(jnp.float32)).astype(jnp.bfloat16)
    weighted = jnp.einsum(
        "sth,sthv->shv", score_high, value_blocks, preferred_element_type=jnp.float32
    )
    weighted = weighted + jnp.einsum(
        "sth,sthv->shv", score_low, value_blocks, preferred_element_type=jnp.float32
    )
    partial_state = factor[..., None] * weighted
    partial_norm = jnp.sum(query_full * scaled_norm, axis=-1)
    query_state, query_norm = lax.psum((partial_state, partial_norm), "sp")
    forget_new = jax.nn.log_sigmoid(new_gates[1])
    input_new = new_gates[0]
    mixed = jnp.maximum(forget_new + global_max, input_new)
    carried = jnp.exp(forget_new + global_max - mixed)
    fresh = jnp.exp(input_new - mixed)
    own_score = jnp.sum(query_full * new_key.astype(jnp.float32), axis=-1) * key_scale
    numer = carried[..., None] * query_state + (fresh * own_score)[..., None] * new_value.astype(
        jnp.float32
    )
    denom = carried * query_norm + fresh * own_score
    first_read = (numer / jnp.maximum(jnp.abs(denom), 1.0)[..., None]).astype(jnp.bfloat16)
    return (memory_rows.astype(jnp.bfloat16), norm_rows, global_max, first_read)


def solution(mesh):
    placed = (
        P(None, "sp", None),
        P("sp", "tp"),
        P("sp", "tp"),
        P(),
        P(),
        P(),
        P(),
        P(None, "tp", None),
        P(None, "tp", None),
        P(None, "tp", None),
        P(None, None, "tp"),
    )
    return jax.shard_map(
        chosen,
        mesh=mesh,
        in_specs=placed,
        out_specs=(
            P(None, "tp", "sp", None),
            P(None, "tp", "sp"),
            P(None, "tp"),
            P(None, "tp", None),
        ),
        check_vma=False,
    )
```

```python
import functools
import jax
import jax.numpy as jnp
from jax import lax
from jax.experimental import pallas as pl
from jax.experimental.pallas import tpu as pltpu
from jax.sharding import PartitionSpec as P

HIGH = lax.Precision.HIGHEST
PARTS = 4
KINDS = ("x1", "x2", "x3", "xa", "ya", "xb", "yb", "xc", "yc")
SENDS = 180
SCHEDULE = (
    ("far",),
    ("tx", 0),
    ("px",),
    ("tx", 1),
    ("near",),
    ("x1", 0),
    ("yown",),
    ("tz", 0),
    ("tz", 1),
    ("w", 1),
    ("px2",),
    ("w", 8),
    ("gates",),
    ("x1", 1),
    ("mid",),
    ("tx", 2),
    ("tz", 2),
    ("tx", 3),
    ("p",),
    ("tx", 4),
    ("w", 4),
    ("tz", 3),
    ("x2", 0),
    ("w", 9),
    ("w", 3),
    ("tb", 0),
    ("tx", 5),
    ("ta", 0),
    ("x1", 2),
    ("tx", 6),
    ("x2", 1),
    ("x1", 3),
    ("ta", 1),
    ("w", 2),
    ("x3", 0),
    ("tx", 7),
    ("w", 12),
    ("x1", 4),
    ("pm",),
    ("x3", 1),
    ("w", 10),
    ("x1", 5),
    ("mm", 0, 2, (1, 8, 0, 4)),
    ("x2", 2),
    ("x1", 6),
    ("w", 5),
    ("x2", 3),
    ("tb", 1),
    ("w", 14),
    ("xc", 0),
    ("ta", 2),
    ("tell_all",),
    ("w", 11),
    ("x3", 2),
    ("tb", 2),
    ("w", 13),
    ("ta", 3),
    ("x1", 7),
    ("xa", 0),
    ("d", "x1", 0),
    ("d", "x1", 4),
    ("mm", 2, 2, (1, 8, 0, 4)),
    ("xb", 0),
    ("xa", 1),
    ("tb", 3),
    ("mm", 0, 2, (9, 3, 2, 12)),
    ("x3", 3),
    ("mm", 2, 2, (9, 3, 2, 12, 10, 5, 14, 11)),
    ("mm", 0, 2, (10, 5, 14, 11)),
    ("d", "x2", 0),
    ("d", "x3", 0),
    ("mm", 4, 2, (1, 8, 0, 4, 9, 3, 2, 12)),
    ("xc", 1),
    ("yc", 0),
    ("mm", 4, 2, (10, 5, 14, 11)),
    ("w", 7),
    ("yb", 0),
    ("ya", 0),
    ("w", 6),
    ("yb", 1),
    ("xa", 2),
    ("xc", 2),
    ("weigh",),
    ("xb", 1),
    ("xc", 3),
    ("xa", 3),
    ("ya", 1),
    ("xb", 2),
    ("w", 15),
    ("mm", 4, 2, (13, 7, 6, 15)),
    ("mm", 0, 2, (13, 7, 6, 15)),
    ("mm", 2, 2, (13, 7, 6, 15)),
    ("finish", 0, 2, 4, 5),
    ("reduce", 0),
    ("yc", 1),
    ("ya", 2),
    ("d1", "xa", 0),
    ("d1", "ya", 0),
    ("mma", 6, 1, 0),
    ("d1", "xb", 0),
    ("d1", "yb", 0),
    ("d1", "xc", 0),
    ("d1", "yc", 0),
    ("mma", 7, 2, 0),
    ("ya", 3),
    ("yc", 2),
    ("d1", "xa", 1),
    ("d1", "ya", 1),
    ("mma", 6, 1, 1),
    ("d1", "xb", 1),
    ("d1", "yb", 1),
    ("d1", "xc", 1),
    ("d1", "yc", 1),
    ("mma", 7, 2, 1),
    ("yb", 2),
    ("xb", 3),
    ("yc", 3),
    ("d1", "xa", 2),
    ("d1", "ya", 2),
    ("mma", 6, 1, 2),
    ("d1", "xb", 2),
    ("d1", "yb", 2),
    ("d1", "xc", 2),
    ("d1", "yc", 2),
    ("mma", 7, 2, 2),
    ("reduce_on",),
    ("yb", 3),
    ("finish", 1, 3),
    ("d1", "xa", 3),
    ("d1", "ya", 3),
    ("mma", 6, 1, 3),
    ("d1", "xb", 3),
    ("d1", "yb", 3),
    ("d1", "xc", 3),
    ("d1", "yc", 3),
    ("mma", 7, 2, 3),
    ("finish", 6, 7, 8),
    ("reduce", 1),
)


def flip(bit, change):
    return bit + change - 2 * bit * change


def log_sigmoid(v):
    return jnp.minimum(v, 0.0) - jnp.log1p(jnp.exp(-jnp.abs(v)))


def iota(shape, dim):
    return lax.broadcasted_iota(jnp.int32, shape, dim)


def kernel(
    prompt,
    w_key,
    w_value,
    w_igate,
    w_fgate,
    input_bias,
    forget_bias,
    new_query,
    new_key,
    new_value,
    new_gates,
    memory_out,
    norm_out,
    max_out,
    read_out,
    xb,
    wb,
    pass_w,
    acc,
    decay,
    vals,
    weight,
    gate_w,
    stat,
    state,
    late_state,
    pair_state,
    y_in,
    aux,
    pair_aux,
    y_aux,
    rmem,
    raux,
    local_sem,
    ready,
    sends,
    x_recv,
    d_recv,
    w_recv,
    g_recv,
    s_recv,
    y_recv,
    m_recv,
    a_recv,
):
    count = lax.axis_size("sp")
    me = lax.axis_index("sp")
    core = lax.axis_index("tp")
    seqs, span, width = prompt.shape
    depth = w_key.shape[0]
    heads = new_query.shape[1]
    dk = new_query.shape[2]
    dv = new_value.shape[2]
    total_heads = input_bias.shape[1]
    key_scale = dk ** (-0.5)
    cut = width // (2 * PARTS)
    half = span // 2
    rows_out = dk // count
    zh, zl, y, x = me // 8, (me // 4) % 2, (me // 2) % 2, me % 2
    mine = zl * 2 + x
    inner = zh != zl
    outer = zh == zl
    bf16, f32 = jnp.bfloat16, jnp.float32

    def place(dh, dl, dy, dx):
        return flip(zh, dh) * 8 + flip(zl, dl) * 4 + flip(y, dy) * 2 + flip(x, dx)

    sent = []

    def remote(src, dst, recv, sp, tp, when=None):
        copy = pltpu.make_async_remote_copy(
            src_ref=src,
            dst_ref=dst,
            send_sem=sends.at[len(sent)],
            recv_sem=recv,
            device_id=(sp, tp),
            device_id_type=pl.DeviceIdType.MESH,
        )
        sent.append((copy, when))
        return copy

    def start(copies, when=None):
        def run():
            for copy in copies:
                copy.start()

        if when is None:
            run()
        else:
            pl.when(when)(run)

    def landed(ref, sem):
        pltpu.make_async_copy(ref, ref, sem).wait()

    to_x, to_y, to_z = place(0, 0, 0, 1), place(0, 0, 1, 0), place(0, 1, 0, 0)
    to_far, to_mid = place(1, 0, 0, 0), place(1, 1, 0, 0)
    barrier = pltpu.get_barrier_semaphore()

    def tell(sem, sp, tp):
        pl.semaphore_signal(
            sem, inc=1, device_id=(sp, tp), device_id_type=pl.DeviceIdType.MESH
        )

    gate_w[...] = jnp.zeros(gate_w.shape, f32)
    for peer in (to_x, to_y, to_z):
        tell(barrier, peer, core)
    tell(barrier, me, 1 - core)

    @pl.when(inner)
    def _():
        tell(barrier, to_mid, core)

    def bits(slot):
        return slot // 8, (slot // 4) % 2, (slot // 2) % 2, slot % 2

    def w_rows(slot):
        return pl.ds(pl.multiple_of(place(*bits(slot)) * depth, depth), depth)

    def group_cols(dl, dx):
        group = flip(zl, dl) * 2 + flip(x, dx)
        kc = pl.ds(pl.multiple_of(group * dk, dk), dk)
        vc = pl.ds(pl.multiple_of(group * dv, dv), dv)
        return kc, vc

    own_x = []
    for s in range(seqs):
        c = pltpu.make_async_copy(
            prompt.at[s], xb.at[pl.ds(s * span, span)], local_sem.at[s]
        )
        c.start()
        own_x.append(c)
    kc, vc = group_cols(0, 0)
    own_w = [
        pltpu.make_async_copy(w_key.at[:, kc], wb.at[w_rows(0), :dk], local_sem.at[2]),
        pltpu.make_async_copy(w_value.at[:, vc], wb.at[w_rows(0), dk:], local_sem.at[3]),
    ]
    for c in own_w:
        c.start()
    pl.semaphore_wait(barrier, 4 + jnp.where(inner, 1, 0))

    def w_own(dl, dx, peer, slot, when=None):
        kc, vc = group_cols(dl, dx)
        rows = w_rows(0)
        return [
            remote(w_key.at[:, kc], wb.at[rows, :dk], w_recv.at[slot], peer, core, when),
            remote(w_value.at[:, vc], wb.at[rows, dk:], w_recv.at[slot], peer, core, when),
        ]

    def w_relay(slot, peer, there, when=None):
        rows = w_rows(slot)
        return [remote(wb.at[rows], wb.at[rows], w_recv.at[there], peer, core, when)]

    def w_wait(slot):
        landed(wb.at[w_rows(slot)], w_recv.at[slot])

    def columns(owner, k):
        return pl.ds(pl.multiple_of((owner * PARTS + k) * cut, cut), cut)

    def rows_of(kind, unit):
        if kind in ("x1", "x2", "x3"):
            chunk = {"x1": 2 + unit // PARTS, "x2": 4, "x3": 5}[kind]
            return chunk * span, span
        chunk = {"a": 6, "b": 7, "c": 8}[kind[1]]
        return chunk * span + (half if kind[0] == "y" else 0), half

    def part(kind, unit, owner):
        low, size = rows_of(kind, unit)
        return xb.at[pl.ds(low, size), columns(owner, unit % PARTS)]

    def sem(table, kind, unit):
        return table.at[KINDS.index(kind), unit]

    def x_own(s, low, size, kind, unit, peer, when=None):
        src = prompt.at[s, pl.ds(low, size), columns(core, unit % PARTS)]
        copy = remote(src, part(kind, unit, core), sem(x_recv, kind, unit), peer, core, when)
        start([copy], when)

    def x_pass(kind, there, unit, peer, when=None):
        copy = remote(
            part(kind, unit, core),
            part(there, unit, core),
            sem(x_recv, there, unit),
            peer,
            core,
            when,
        )
        start([copy], when)

    def only(kind):
        return inner if kind[1] in "bc" else None

    def x_across(kind, unit):
        own = part(kind, unit, core)
        when = only(kind)
        start([remote(own, own, sem(d_recv, kind, unit), me, 1 - core, when)], when)

    def maybe(when, run):
        if when is None:
            run()
        else:
            pl.when(when)(run)

    def x_wait(kind, unit):
        maybe(
            only(kind),
            lambda: landed(part(kind, unit, core), sem(x_recv, kind, unit)),
        )

    def d_wait(kind, unit):
        maybe(
            only(kind),
            lambda: landed(part(kind, unit, 1 - core), sem(d_recv, kind, unit)),
        )

    def go_x(kind, unit):
        x_wait(kind, unit)
        if kind == "x2":
            x_pass("x2", "x3", unit, to_x)
        if kind == "xa":
            x_pass("xa", "ya", unit, to_x, outer if unit >= PARTS // 2 else None)
        if kind == "xc":
            x_pass("xc", "yc", unit, to_x, inner)
        if kind == "x1" and unit >= PARTS:
            k = unit - PARTS
            src = xb.at[pl.ds(3 * span + half, half), columns(core, k)]
            dst = part("yb", k, core)
            start([remote(src, dst, sem(x_recv, "yb", k), to_z, core, outer)], outer)
            if k >= PARTS // 2:
                src = xb.at[pl.ds(3 * span, half), columns(core, k)]
                dst = part("ya", k, core)
                start([remote(src, dst, sem(x_recv, "ya", k), to_z, core, outer)], outer)
        x_across(kind, unit)

    def go_w(slot):
        w_wait(slot)
        start(w_relay(slot, to_y, slot + 2))

    first = core == 0

    near, far, mid = (
        w_own(1, 0, to_z, 4),
        w_own(0, 0, to_far, 8),
        w_own(1, 0, to_mid, 12, inner),
    )
    px, y_own = w_own(0, 1, to_x, 1), w_own(0, 0, to_y, 2)
    kc, vc = group_cols(1, 1)
    px2 = [
        remote(w_key.at[:, kc], pass_w.at[:, :dk], w_recv.at[0], to_x, core),
        remote(w_value.at[:, vc], pass_w.at[:, dk:], w_recv.at[0], to_x, core),
    ]

    def greet():
        @pl.when(inner)
        def _():
            tell(ready, to_z, core)
            tell(ready, to_mid, core)

        pl.semaphore_wait(ready, 1)

    w_gate = jnp.concatenate([w_igate[...], w_fgate[...]], axis=0)
    square = iota((total_heads, total_heads), 0) == iota((total_heads, total_heads), 1)

    def upright(row):
        return jnp.sum(jnp.where(square, row, 0.0), axis=1, keepdims=True)

    bias_in, bias_f = upright(input_bias[...]), upright(forget_bias[...])
    after = (iota((span, span), 0) > iota((span, span), 1)).astype(f32)
    spot_head = iota((total_heads, 128), 0) - core * heads
    spot_lane = iota((total_heads, 128), 1)
    local_head = (spot_head >= 0) & (spot_head < heads)
    def gates():
        for c in own_x:
            c.wait()
        packed = jnp.zeros((1, 128), f32)
        for s in range(seqs):
            both = lax.dot_general(
                w_gate,
                xb[s * span : (s + 1) * span],
                (((1,), (1,)), ((), ())),
                preferred_element_type=f32,
            )
            gate_in = both[:total_heads] + bias_in
            forget = log_sigmoid(both[total_heads:] + bias_f)
            level = gate_in + jnp.dot(forget, after, precision=HIGH, preferred_element_type=f32)
            top = jnp.max(level, axis=1, keepdims=True)
            total = jnp.sum(forget, axis=1, keepdims=True)
            part_w = jnp.exp(level - top) * key_scale
            gate_w[0, s * heads : (s + 1) * heads, :span] = jnp.where(
                first, part_w[:heads], part_w[heads : 2 * heads]
            )
            at = spot_lane - s * heads
            packed = packed + jnp.sum(
                jnp.where(local_head & (at == spot_head), total, 0.0)
                + jnp.where(local_head & (at - seqs * heads == spot_head), top, 0.0),
                axis=0,
                keepdims=True,
            )
        stat[me] = jnp.broadcast_to(packed, (8, 128))
        for c in own_w:
            c.wait()

    def tell_all():
        for off in range(count - 1, 0, -1):
            peer = place(*bits(off))
            start([remote(stat.at[me], stat.at[me], s_recv, peer, core)])
        for block, peer in ((1, to_x), (2, to_z), (3, place(0, 1, 0, 1))):
            start([remote(gate_w.at[0], gate_w.at[block], g_recv.at[block], peer, core)])
        for block, peer in ((4, to_mid), (5, place(1, 1, 0, 1))):
            copy = remote(
                gate_w.at[0], gate_w.at[block], g_recv.at[block], peer, core, inner
            )
            start([copy], inner)

    def choose(i, values):
        out = jnp.int32(values[0])
        for k, v in enumerate(values[1:], 1):
            out = jnp.where(i == k, v, out)
        return out

    def multiply(low, size, slots):
        width_in = 4 if len(slots) % 4 == 0 else 2

        def step(i, carry):
            out = None
            for off in range(width_in):
                rows = w_rows(choose(i, slots[off::width_in]))
                piece = jnp.dot(
                    xb[pl.ds(low, size), rows], wb[rows], preferred_element_type=f32
                )
                out = piece if out is None else out + piece
            acc[pl.ds(low, size)] += out
            return carry

        lax.fori_loop(0, len(slots) // width_in, step, 0)

    def multiply_part(low, size, k):
        out = None
        for owner in range(2):
            cols = slice((owner * PARTS + k) * cut, (owner * PARTS + k + 1) * cut)
            piece = jnp.dot(xb[low : low + size, cols], wb[cols], preferred_element_type=f32)
            out = piece if out is None else out + piece
        acc[low : low + size] += out

    def zero(i, carry):
        acc[pl.ds(pl.multiple_of(i * span, span), span)] = jnp.zeros((span, dk + dv), f32)
        return carry

    lax.fori_loop(0, 9, zero, 0)

    eye = (iota((span, span), 0) == iota((span, span), 1)).astype(f32)
    here = iota((span, seqs * heads), 1)
    chip = iota((count, seqs * heads), 0)
    lane16 = iota((count, seqs * heads), 1)

    def weigh():
        landed(stat.at[pl.ds(0, count - 1)], s_recv)
        table = jnp.concatenate([stat[c, 0:1] for c in range(count)], axis=0)
        beyond = (iota((count, count), 1) > iota((count, count), 0)).astype(f32)
        later = jnp.dot(beyond, table, precision=HIGH, preferred_element_type=f32)
        lift = later[:, : seqs * heads] + table[:, seqs * heads : 2 * seqs * heads]
        highest = jnp.max(lift, axis=0, keepdims=True)
        factor = jnp.exp(lift - highest)
        weight[8 * span : 9 * span] = jnp.zeros((span, 128), f32)

        def column(block, s):
            turned = lax.dot_general(
                eye,
                gate_w[block][:, :span],
                (((1,), (1,)), ((), ())),
                precision=HIGH,
                preferred_element_type=f32,
            )
            dh, pos = (0, block) if block < 4 else (1, 2 + block % 2)
            lane = s * heads + mine
            hit = (chip == place(dh, pos // 2, 0, pos % 2)) & (lane16 == lane)
            scale = jnp.sum(jnp.where(hit, factor, 0.0), keepdims=True)
            one = jnp.sum(jnp.where(here == lane, turned, 0.0), axis=1, keepdims=True)
            return jnp.broadcast_to(one * scale, (span, 128))

        for block in range(4):
            if block:
                landed(gate_w.at[block], g_recv.at[block])
            weight[pl.ds((2 * block if block < 2 else 2 + block) * span, span)] = column(block, 0)
            late = column(block, 1)
            if block < 2:
                weight[pl.ds((2 * block + 1) * span, span)] = late
            else:
                for chunk in (6, 7):
                    low = chunk * span + (block - 2) * half
                    weight[pl.ds(low, half)] = late[(chunk - 6) * half : (chunk - 5) * half]

        @pl.when(inner)
        def _():
            for block in (4, 5):
                landed(gate_w.at[block], g_recv.at[block])
                low = 8 * span + (block - 4) * half
                weight[pl.ds(low, half)] = column(block, 1)[half:]

        return highest

    to_chunk = (0, 4, 1, 5, 2, 3, 6, 7, 8)

    def finish(chunk):
        rows = slice(chunk * span, (chunk + 1) * span)
        to = slice(to_chunk[chunk] * span, (to_chunk[chunk] + 1) * span)
        keys = acc[rows, :dk].astype(bf16).astype(f32)
        decay[to] = (weight[rows, 0:1] * keys).astype(bf16)
        vals[to] = acc[rows, dk:].astype(bf16)

    pick = iota((heads, dk), 0) == mine

    def out_rows(chip):
        return pl.ds(pl.multiple_of(chip * rows_out, rows_out), rows_out)

    def reduce(s):
        span_rows = slice(0, 4 * span) if s == 0 else slice(4 * span, 9 * span)
        d = decay[span_rows]
        ones = jnp.ones((8, d.shape[0]), bf16)
        sums = lax.dot_general(
            d, vals[span_rows], (((0,), (0,)), ((), ())), preferred_element_type=f32
        )
        high = sums.astype(bf16)
        if s == 0:
            for block in range(count // 2):
                low = (block // 2) * 2 * rows_out
                state[block % 2, low : low + 2 * rows_out] = high[
                    block * 2 * rows_out : (block + 1) * 2 * rows_out
                ]
            start([remote(state.at[1 - y], y_in, y_recv.at[0], to_y, core)])
        else:
            late_state[...] = high
            for off in range(count - 1, 0, -1):
                peer = place(*bits(off))
                src = late_state.at[out_rows(peer)]
                start([remote(src, rmem.at[1, me], m_recv.at[1], peer, core)])
        low = (sums - high.astype(f32)).astype(bf16)
        norms = jnp.dot(ones, d, preferred_element_type=f32)
        query = jnp.sum(
            jnp.where(pick, new_query[s].astype(f32), 0.0), axis=0, keepdims=True
        )
        wide = jnp.broadcast_to(query, (8, dk)).astype(bf16)
        seen = jnp.dot(wide, high, preferred_element_type=f32) + jnp.dot(
            wide, low, preferred_element_type=f32
        )
        for k in range(dv // 128):
            aux[s, k : k + 1] = seen[0:1, k * 128 : (k + 1) * 128]
        for k in range(dk // 128):
            aux[s, 4 + k : 5 + k] = norms[0:1, k * 128 : (k + 1) * 128]
        dot_norm = jnp.sum(query * norms[0:1], axis=1, keepdims=True)
        aux[s, 6:8] = jnp.broadcast_to(dot_norm, (2, 128))
        if s == 0:
            start([remote(aux.at[0], y_aux, y_recv.at[1], to_y, core)])
        else:
            for off in range(count - 1, 0, -1):
                peer = place(*bits(off))
                start([remote(aux.at[1], raux.at[1, me], a_recv.at[1], peer, core)])
            rmem[1, me] = late_state[out_rows(me)]
            raux[1, me] = aux[1]

    spot8 = (zh * 2 + zl) * 2 + x

    def reduce_on():
        landed(y_in, y_recv.at[0])
        pair_state[...] = (state[y].astype(f32) + y_in[...].astype(f32)).astype(bf16)
        landed(y_aux, y_recv.at[1])
        pair_aux[...] = aux[0] + y_aux[...]
        for off in range(count // 2 - 1, 0, -1):
            dh, dl, dx = off // 4, (off // 2) % 2, off % 2
            peer = place(dh, dl, 0, dx)
            spot = (flip(zh, dh) * 2 + flip(zl, dl)) * 2 + flip(x, dx)
            src = pair_state.at[out_rows(spot)]
            start([remote(src, rmem.at[0, spot8], m_recv.at[0], peer, core)])
            start([remote(pair_aux, raux.at[0, spot8], a_recv.at[0], peer, core)])
        rmem[0, spot8] = pair_state[out_rows(spot8)]
        raux[0, spot8] = pair_aux[...]

    streams = {"px": px, "px2": px2, "yown": y_own, "near": near}
    highest = None
    for name, *arg in SCHEDULE:
        if name in streams:
            start(streams[name])
        elif name == "far":
            greet()
            start(far)
        elif name == "mid":
            start(mid, inner)
        elif name == "gates":
            gates()
        elif name == "tell_all":
            tell_all()
        elif name == "tx":
            x_own(arg[0] // PARTS, 0, span, "x1", arg[0], to_x)
        elif name == "tz":
            x_own(0, 0, span, "x2", arg[0], to_z)
        elif name == "ta":
            x_own(1, 0, half, "xa", arg[0], to_z)
        elif name == "tb":
            x_own(1, half, half, "xb", arg[0], to_z, outer)
            x_own(1, half, half, "xc", arg[0], to_mid, inner)
        elif name == "w":
            slot = arg[0]
            w_wait(slot)
            if slot == 1:
                start(w_relay(1, to_far, 9))
            if slot % 4 < 2:
                start(w_relay(slot, to_y, slot + 2))
            if slot in (4, 5):
                start(w_relay(slot, to_far, slot + 8, inner), inner)
        elif name == "p":
            landed(pass_w, w_recv.at[0])
            start([remote(pass_w, wb.at[w_rows(1)], w_recv.at[5], to_z, core)])
        elif name == "pm":
            copy = remote(pass_w, wb.at[w_rows(1)], w_recv.at[13], to_mid, core, inner)
            start([copy], inner)
        elif name in KINDS:
            go_x(name, arg[0])
        elif name == "d":
            kind, low = arg
            for unit in range(low, low + PARTS):
                d_wait(kind, unit)
        elif name == "mm":
            low, chunks, slots = arg
            maybe(
                inner if low >= 7 else None,
                lambda: multiply(low * span, chunks * span, slots),
            )
        elif name == "d1":
            d_wait(*arg)
        elif name == "mma":
            low, chunks, k = arg
            maybe(
                inner if low >= 7 else None,
                lambda: multiply_part(low * span, chunks * span, k),
            )
        elif name == "weigh":
            highest = weigh()
        elif name == "finish":
            for chunk in arg:
                finish(chunk)
        elif name == "reduce":
            reduce(arg[0])
        elif name == "reduce_on":
            reduce_on()

    def stack(ref):
        return jnp.concatenate([ref[s].astype(f32) for s in range(seqs)], axis=0)

    queries = stack(new_query)
    own = jnp.sum(queries * stack(new_key), axis=1, keepdims=True) * key_scale
    own_head = iota((seqs * heads, heads), 0) % heads == iota((seqs * heads, heads), 1)

    def gate_column(block):
        wide = jnp.concatenate(
            [jnp.broadcast_to(block[s : s + 1], (heads, heads)) for s in range(seqs)], axis=0
        )
        return jnp.sum(jnp.where(own_head, wide, 0.0), axis=1, keepdims=True)

    gate_in, gate_f = gate_column(new_gates[0]), log_sigmoid(gate_column(new_gates[1]))
    token_values = stack(new_value)
    top = upright(highest)
    max_out[...] = top

    read_rows, norm_rows, dot_rows = [], [], []
    for s in range(seqs):
        peers = count // 2 - 1 if s == 0 else count - 1
        landed(rmem.at[s, pl.ds(0, peers)], m_recv.at[s])
        landed(raux.at[s, pl.ds(0, peers)], a_recv.at[s])
        for h in range(heads):
            if s == 0:
                srcs = [(a * 2 + h // 2) * 2 + h % 2 for a in range(2)]
            else:
                srcs = [
                    (a * 2 + h // 2) * 4 + b * 2 + h % 2 for a in range(2) for b in range(2)
                ]
            mem = rmem[s, srcs[0]].astype(f32)
            both = raux[s, srcs[0]]
            for src in srcs[1:]:
                mem = mem + rmem[s, src].astype(f32)
                both = both + raux[s, src]
            memory_out[s, h] = mem.astype(bf16)
            read_rows.append(
                jnp.concatenate([both[k : k + 1] for k in range(dv // 128)], 1)
            )
            norm_rows.append(
                jnp.concatenate([both[4 + k : 5 + k] for k in range(dk // 128)], 1)
            )
            dot_rows.append(both[6:7, 0:1])
    query_state = jnp.concatenate(read_rows, axis=0)
    norm_all = jnp.concatenate(norm_rows, axis=0)
    query_norm = jnp.concatenate(dot_rows, axis=0)
    take = (
        iota((dk, rows_out), 0) == me * rows_out + iota((dk, rows_out), 1)
    ).astype(f32)
    norm_out[...] = jnp.dot(norm_all, take, precision=HIGH, preferred_element_type=f32)
    mixed = jnp.maximum(gate_f + top, gate_in)
    carried = jnp.exp(gate_f + top - mixed)
    fresh = jnp.exp(gate_in - mixed)
    numer = carried * query_state + (fresh * own) * token_values
    denom = carried * query_norm + fresh * own
    read_out[...] = (numer / jnp.maximum(jnp.abs(denom), 1.0)).astype(bf16)
    for copy, when in sent:
        if when is None:
            copy.wait_send()
        else:
            pl.when(when)(copy.wait_send)


def hand_on(memory, norm, top, read, memory_out, norm_out, max_out, read_out):
    seqs, heads = max_out.shape
    memory_out[...] = memory[...]
    at = lax.broadcasted_iota(jnp.int32, (seqs * heads, heads), 0)
    to = lax.broadcasted_iota(jnp.int32, (seqs * heads, heads), 1)
    wide = read[...].astype(jnp.float32)
    for s in range(seqs):
        rows = slice(s * heads, (s + 1) * heads)
        norm_out[s] = norm[rows]
        read_out[s] = wide[rows].astype(jnp.bfloat16)
        max_out[s : s + 1] = jnp.sum(
            jnp.where(at == s * heads + to, top[...], 0.0), axis=0, keepdims=True
        )


def by_head(
    prompt,
    w_key,
    w_value,
    w_igate,
    w_fgate,
    input_bias,
    forget_bias,
    new_query,
    new_key,
    new_value,
    new_gates,
):
    count = lax.axis_size("sp")
    seqs, span, width = prompt.shape
    depth = w_key.shape[0]
    heads, dk = new_query.shape[1:]
    dv = new_value.shape[2]
    rows = seqs * span
    vmem = pl.BlockSpec(memory_space=pltpu.VMEM)
    hbm = pl.BlockSpec(memory_space=pl.ANY)
    dma = pltpu.SemaphoreType.DMA
    memory, norm, top, read = pl.pallas_call(
        kernel,
        out_shape=(
            jax.ShapeDtypeStruct((seqs, heads, dk // count, dv), jnp.bfloat16),
            jax.ShapeDtypeStruct((seqs * heads, dk // count), jnp.float32),
            jax.ShapeDtypeStruct((seqs * heads, 1), jnp.float32),
            jax.ShapeDtypeStruct((seqs * heads, dv), jnp.bfloat16),
        ),
        in_specs=[hbm, hbm, hbm] + [vmem] * 8,
        out_specs=(vmem, vmem, vmem, vmem),
        scratch_shapes=[
            pltpu.VMEM((9 * span, width), jnp.bfloat16),
            pltpu.VMEM((width, dk + dv), jnp.bfloat16),
            pltpu.VMEM((depth, dk + dv), jnp.bfloat16),
            pltpu.VMEM((9 * span, dk + dv), jnp.float32),
            pltpu.VMEM((9 * span, dk), jnp.bfloat16),
            pltpu.VMEM((9 * span, dv), jnp.bfloat16),
            pltpu.VMEM((9 * span, 128), jnp.float32),
            pltpu.VMEM((6, 8, 256), jnp.float32),
            pltpu.VMEM((count, 8, 128), jnp.float32),
            pltpu.VMEM((2, dk // 2, dv), jnp.bfloat16),
            pltpu.VMEM((dk, dv), jnp.bfloat16),
            pltpu.VMEM((dk // 2, dv), jnp.bfloat16),
            pltpu.VMEM((dk // 2, dv), jnp.bfloat16),
            pltpu.VMEM((seqs, 8, 128), jnp.float32),
            pltpu.VMEM((8, 128), jnp.float32),
            pltpu.VMEM((8, 128), jnp.float32),
            pltpu.VMEM((seqs, count, dk // count, dv), jnp.bfloat16),
            pltpu.VMEM((seqs, count, 8, 128), jnp.float32),
            dma((4,)),
            pltpu.SemaphoreType.REGULAR,
            dma((SENDS,)),
            dma((len(KINDS), 2 * PARTS)),
            dma((len(KINDS), 2 * PARTS)),
            dma((16,)),
            dma((6,)),
            dma,
            dma((2,)),
            dma((seqs,)),
            dma((seqs,)),
        ],
        compiler_params=pltpu.CompilerParams(
            collective_id=0, has_side_effects=True, vmem_limit_bytes=60 * 1024 * 1024
        ),
    )(
        prompt,
        w_key,
        w_value,
        w_igate.T,
        w_fgate.T,
        input_bias[None],
        forget_bias[None],
        new_query,
        new_key,
        new_value,
        new_gates,
    )
    return pl.pallas_call(
        hand_on,
        out_shape=(
            jax.ShapeDtypeStruct((seqs, heads, dk // count, dv), jnp.bfloat16),
            jax.ShapeDtypeStruct((seqs, heads, dk // count), jnp.float32),
            jax.ShapeDtypeStruct((seqs, heads), jnp.float32),
            jax.ShapeDtypeStruct((seqs, heads, dv), jnp.bfloat16),
        ),
        in_specs=[vmem] * 4,
        out_specs=(vmem,) * 4,
    )(memory, norm, top, read)


def chosen(*args):
    prompt, new_query, new_value = args[0], args[7], args[9]
    heads = new_query.shape[1]
    count = lax.axis_size("sp")
    fits = (
        lax.axis_size("tp") == 2
        and heads == 4
        and count == 16
        and prompt.shape[0] == 2
        and new_query.shape[2] == 256
        and new_value.shape[2] == 512
    )
    return by_head(*args) if fits else per_device(*args)


def entering(value, axis, join, neutral):
    count, mine = (lax.axis_size(axis), lax.axis_index(axis))
    pieces = lax.all_gather(value, axis)
    pieces = pieces[::-1]
    mine = count - 1 - mine
    so_far = jnp.full_like(value, 0) + jnp.asarray(neutral, value.dtype)

    def turn(position, so_far):
        longer = join(so_far, pieces[position])
        return jnp.where(position < mine, longer, so_far)

    return lax.fori_loop(0, count - 1, turn, so_far)


def add_pair(earlier, later):
    return earlier + later


def per_device(
    prompt,
    w_key,
    w_value,
    w_igate,
    w_fgate,
    input_bias,
    forget_bias,
    new_query,
    new_key,
    new_value,
    new_gates,
):
    seq_count, span_len, model_width = prompt.shape
    local_heads = new_query.shape[1]
    key_size = new_query.shape[2]
    value_size = new_value.shape[2]
    key_scale = key_size ** (-0.5)
    token_rows = prompt.reshape(seq_count * span_len, model_width)
    whole_key, whole_value = (
        lax.all_gather(w_key, "sp", axis=0, tiled=True),
        lax.all_gather(w_value, "sp", axis=0, tiled=True),
    )
    key_rows = jnp.dot(token_rows, whole_key, preferred_element_type=jnp.float32).astype(
        jnp.bfloat16
    )
    value_rows = jnp.dot(token_rows, whole_value, preferred_element_type=jnp.float32).astype(
        jnp.bfloat16
    )
    head_start = lax.axis_index("tp") * local_heads
    input_all = jnp.dot(token_rows, w_igate, preferred_element_type=jnp.float32) + input_bias
    forget_all = jnp.dot(token_rows, w_fgate, preferred_element_type=jnp.float32) + forget_bias
    input_gate = lax.dynamic_slice_in_dim(input_all, head_start, local_heads, 1).reshape(
        seq_count, span_len, local_heads
    )
    log_forget = jax.nn.log_sigmoid(
        lax.dynamic_slice_in_dim(forget_all, head_start, local_heads, 1)
    ).reshape(seq_count, span_len, local_heads)
    block_total = jnp.sum(log_forget, axis=1)
    forget_after = block_total[:, None] - jnp.cumsum(log_forget, axis=1)
    log_weight = forget_after + input_gate
    block_max = jnp.max(log_weight, axis=1)
    key_blocks = key_rows.reshape(seq_count, span_len, local_heads, key_size).astype(jnp.float32)
    decayed = (jnp.exp(log_weight - block_max[:, None])[..., None] * key_scale * key_blocks).astype(
        jnp.bfloat16
    )
    value_blocks = value_rows.reshape(seq_count, span_len, local_heads, value_size)
    block_norm = jnp.sum(decayed.astype(jnp.float32), axis=1)
    later_total = entering(block_total, "sp", add_pair, jnp.zeros_like(block_total))
    block_lift = later_total + block_max
    global_max = lax.pmax(block_lift, "sp")
    factor = jnp.exp(block_lift - global_max)
    scaled_norm = factor[:, :, None] * block_norm
    query_full = new_query.astype(jnp.float32)
    block_state = jnp.einsum(
        "sthk,sthv->shkv", decayed, value_blocks, preferred_element_type=jnp.float32
    )
    scaled_state = factor[:, :, None, None] * block_state
    memory_rows, norm_rows = (
        lax.psum_scatter(scaled_state, "sp", scatter_dimension=2, tiled=True),
        lax.psum_scatter(scaled_norm, "sp", scatter_dimension=2, tiled=True),
    )
    token_score = jnp.einsum(
        "shk,sthk->sth", new_query, decayed, preferred_element_type=jnp.float32
    )
    score_high = token_score.astype(jnp.bfloat16)
    score_low = (token_score - score_high.astype(jnp.float32)).astype(jnp.bfloat16)
    weighted = jnp.einsum(
        "sth,sthv->shv", score_high, value_blocks, preferred_element_type=jnp.float32
    )
    weighted = weighted + jnp.einsum(
        "sth,sthv->shv", score_low, value_blocks, preferred_element_type=jnp.float32
    )
    partial_state = factor[..., None] * weighted
    partial_norm = jnp.sum(query_full * scaled_norm, axis=-1)
    query_state, query_norm = lax.psum((partial_state, partial_norm), "sp")
    forget_new = jax.nn.log_sigmoid(new_gates[1])
    input_new = new_gates[0]
    mixed = jnp.maximum(forget_new + global_max, input_new)
    carried = jnp.exp(forget_new + global_max - mixed)
    fresh = jnp.exp(input_new - mixed)
    own_score = jnp.sum(query_full * new_key.astype(jnp.float32), axis=-1) * key_scale
    numer = carried[..., None] * query_state + (fresh * own_score)[..., None] * new_value.astype(
        jnp.float32
    )
    denom = carried * query_norm + fresh * own_score
    first_read = (numer / jnp.maximum(jnp.abs(denom), 1.0)[..., None]).astype(jnp.bfloat16)
    return (memory_rows.astype(jnp.bfloat16), norm_rows, global_max, first_read)


def solution(mesh):
    placed = (
        P(None, "sp", None),
        P("sp", "tp"),
        P("sp", "tp"),
        P(),
        P(),
        P(),
        P(),
        P(None, "tp", None),
        P(None, "tp", None),
        P(None, "tp", None),
        P(None, None, "tp"),
    )
    return jax.shard_map(
        chosen,
        mesh=mesh,
        in_specs=placed,
        out_specs=(
            P(None, "tp", "sp", None),
            P(None, "tp", "sp"),
            P(None, "tp"),
            P(None, "tp", None),
        ),
        check_vma=False,
    )
```

```python
import functools
import jax
import jax.numpy as jnp
from jax import lax
from jax.experimental import pallas as pl
from jax.experimental.pallas import tpu as pltpu
from jax.sharding import PartitionSpec as P

HIGH = lax.Precision.HIGHEST
PARTS = 4
KINDS = ("x1", "x2", "x3", "xa", "ya", "xb", "yb", "xc", "yc")
SENDS = 212
SCHEDULE = (
    ("far", 0),
    ("tx", 0),
    ("px", 0),
    ("near", 0),
    ("tx", 1),
    ("px2", 0),
    ("mid", 0),
    ("tz", 0),
    ("yown", 0),
    ("near", 1),
    ("px", 1),
    ("tb", 0),
    ("yown", 1),
    ("w", 4, 0),
    ("px2", 1),
    ("w", 1, 0),
    ("x1", 0),
    ("p", 0),
    ("w", 8, 0),
    ("x2", 0),
    ("tx", 2),
    ("mid", 1),
    ("w", 1, 1),
    ("gates",),
    ("w", 4, 1),
    ("tx", 3),
    ("w", 12, 0),
    ("tx", 4),
    ("pm", 0),
    ("tz", 1),
    ("p", 1),
    ("w", 5, 0),
    ("x2", 1),
    ("x1", 1),
    ("w", 2, 0),
    ("w", 9, 0),
    ("tz", 2),
    ("pm", 1),
    ("tx", 5),
    ("tz", 3),
    ("w", 5, 1),
    ("far", 1),
    ("mm", 0, 2, (1, 0, 4, 5)),
    ("x1", 2),
    ("x1", 3),
    ("w", 9, 1),
    ("x1", 4),
    ("tx", 6),
    ("x2", 2),
    ("w", 7, 0),
    ("ta", 0),
    ("w", 3, 0),
    ("x3", 0),
    ("w", 12, 1),
    ("w", 7, 1),
    ("tx", 7),
    ("w", 14, 0),
    ("w", 6, 1),
    ("x1", 5),
    ("w", 10, 0),
    ("tell_all",),
    ("ta", 1),
    ("xb", 0),
    ("ta", 2),
    ("x2", 3),
    ("w", 11, 0),
    ("x1", 6),
    ("w", 6, 0),
    ("w", 2, 1),
    ("ta", 3),
    ("w", 3, 1),
    ("w", 13, 0),
    ("yb", 0),
    ("w", 11, 1),
    ("mm", 0, 2, (9, 12, 7, 6)),
    ("tb", 1),
    ("w", 13, 1),
    ("yb", 1),
    ("xc", 0),
    ("mm", 0, 2, (2, 3, 11, 13)),
    ("tb", 2),
    ("x1", 7),
    ("x3", 1),
    ("w", 15, 0),
    ("w", 8, 1),
    ("w", 14, 1),
    ("xa", 0),
    ("d", "x1", 0),
    ("d", "x1", 4),
    ("mm", 2, 2, (1, 0, 4, 5, 9, 12, 7, 6)),
    ("x3", 2),
    ("yb", 2),
    ("mm", 2, 2, (2, 3, 11, 13)),
    ("tb", 3),
    ("x3", 3),
    ("xa", 1),
    ("weigh",),
    ("xa", 2),
    ("d", "x2", 0),
    ("d", "x3", 0),
    ("mm", 4, 2, (1, 0, 4, 5, 9, 12, 7, 6, 2, 3, 11, 13)),
    ("xc", 1),
    ("xa", 3),
    ("w", 15, 1),
    ("w", 10, 1),
    ("mm", 2, 2, (8, 14, 15, 10)),
    ("mm", 0, 2, (8, 14, 15, 10)),
    ("xc", 2),
    ("mm", 4, 2, (8, 14, 15, 10)),
    ("finish", 0, 2, 4, 5),
    ("reduce", 0),
    ("xb", 1),
    ("ya", 0),
    ("yc", 0),
    ("xc", 3),
    ("yb", 3),
    ("yc", 1),
    ("d1", "xa", 0),
    ("d1", "ya", 0),
    ("mma", 6, 1, 0),
    ("d1", "xb", 0),
    ("d1", "yb", 0),
    ("d1", "xc", 0),
    ("d1", "yc", 0),
    ("mma", 7, 2, 0),
    ("ya", 1),
    ("d1", "xa", 1),
    ("d1", "ya", 1),
    ("mma", 6, 1, 1),
    ("d1", "xb", 1),
    ("d1", "yb", 1),
    ("d1", "xc", 1),
    ("d1", "yc", 1),
    ("mma", 7, 2, 1),
    ("ya", 2),
    ("ya", 3),
    ("xb", 2),
    ("yc", 2),
    ("yc", 3),
    ("reduce_on",),
    ("xb", 3),
    ("d1", "xa", 2),
    ("d1", "ya", 2),
    ("mma", 6, 1, 2),
    ("d1", "xb", 2),
    ("d1", "yb", 2),
    ("d1", "xc", 2),
    ("d1", "yc", 2),
    ("mma", 7, 2, 2),
    ("finish", 1, 3),
    ("d1", "xa", 3),
    ("d1", "ya", 3),
    ("mma", 6, 1, 3),
    ("d1", "xb", 3),
    ("d1", "yb", 3),
    ("d1", "xc", 3),
    ("d1", "yc", 3),
    ("mma", 7, 2, 3),
    ("finish", 6, 7, 8),
    ("reduce", 1),
)


def flip(bit, change):
    return bit + change - 2 * bit * change


def log_sigmoid(v):
    return jnp.minimum(v, 0.0) - jnp.log1p(jnp.exp(-jnp.abs(v)))


def iota(shape, dim):
    return lax.broadcasted_iota(jnp.int32, shape, dim)


def kernel(
    prompt,
    w_key,
    w_value,
    w_igate,
    w_fgate,
    input_bias,
    forget_bias,
    new_query,
    new_key,
    new_value,
    new_gates,
    memory_out,
    norm_out,
    max_out,
    read_out,
    xb,
    wb,
    pass_w,
    acc,
    decay,
    vals,
    weight,
    gate_w,
    stat,
    state,
    late_state,
    pair_state,
    y_in,
    aux,
    pair_aux,
    y_aux,
    rmem,
    raux,
    local_sem,
    ready,
    sends,
    x_recv,
    d_recv,
    w_recv,
    g_recv,
    s_recv,
    y_recv,
    m_recv,
    a_recv,
):
    count = lax.axis_size("sp")
    me = lax.axis_index("sp")
    core = lax.axis_index("tp")
    seqs, span, width = prompt.shape
    depth = w_key.shape[0]
    heads = new_query.shape[1]
    dk = new_query.shape[2]
    dv = new_value.shape[2]
    total_heads = input_bias.shape[1]
    key_scale = dk ** (-0.5)
    cut = width // (2 * PARTS)
    half = span // 2
    rows_out = dk // count
    zh, zl, y, x = me // 8, (me // 4) % 2, (me // 2) % 2, me % 2
    mine = zl * 2 + x
    inner = zh != zl
    outer = zh == zl
    bf16, f32 = jnp.bfloat16, jnp.float32

    def place(dh, dl, dy, dx):
        return flip(zh, dh) * 8 + flip(zl, dl) * 4 + flip(y, dy) * 2 + flip(x, dx)

    sent = []

    def remote(src, dst, recv, sp, tp, when=None):
        copy = pltpu.make_async_remote_copy(
            src_ref=src,
            dst_ref=dst,
            send_sem=sends.at[len(sent)],
            recv_sem=recv,
            device_id=(sp, tp),
            device_id_type=pl.DeviceIdType.MESH,
        )
        sent.append((copy, when))
        return copy

    def start(copies, when=None):
        def run():
            for copy in copies:
                copy.start()

        if when is None:
            run()
        else:
            pl.when(when)(run)

    def landed(ref, sem):
        pltpu.make_async_copy(ref, ref, sem).wait()

    to_x, to_y, to_z = place(0, 0, 0, 1), place(0, 0, 1, 0), place(0, 1, 0, 0)
    to_far, to_mid = place(1, 0, 0, 0), place(1, 1, 0, 0)
    barrier = pltpu.get_barrier_semaphore()

    def tell(sem, sp, tp):
        pl.semaphore_signal(
            sem, inc=1, device_id=(sp, tp), device_id_type=pl.DeviceIdType.MESH
        )

    gate_w[...] = jnp.zeros(gate_w.shape, f32)
    for peer in (to_x, to_y, to_z):
        tell(barrier, peer, core)
    tell(barrier, me, 1 - core)

    @pl.when(inner)
    def _():
        tell(barrier, to_mid, core)

    def bits(slot):
        return slot // 8, (slot // 4) % 2, (slot // 2) % 2, slot % 2

    def w_rows(slot):
        return pl.ds(pl.multiple_of(place(*bits(slot)) * depth, depth), depth)

    def group_cols(dl, dx):
        group = flip(zl, dl) * 2 + flip(x, dx)
        kc = pl.ds(pl.multiple_of(group * dk, dk), dk)
        vc = pl.ds(pl.multiple_of(group * dv, dv), dv)
        return kc, vc

    own_x = []
    for s in range(seqs):
        c = pltpu.make_async_copy(
            prompt.at[s], xb.at[pl.ds(s * span, span)], local_sem.at[s]
        )
        c.start()
        own_x.append(c)
    kc, vc = group_cols(0, 0)
    own_w = [
        pltpu.make_async_copy(w_key.at[:, kc], wb.at[w_rows(0), :dk], local_sem.at[2]),
        pltpu.make_async_copy(w_value.at[:, vc], wb.at[w_rows(0), dk:], local_sem.at[3]),
    ]
    for c in own_w:
        c.start()
    pl.semaphore_wait(barrier, 4 + jnp.where(inner, 1, 0))

    piece = depth // 2

    def w_part(slot, k):
        low = place(*bits(slot)) * depth + k * piece
        return pl.ds(pl.multiple_of(low, piece), piece)

    def w_sem(slot, k):
        return w_recv.at[2 * slot + k]

    def w_own(dl, dx, peer, slot, k, when=None):
        kc, vc = group_cols(dl, dx)
        src, dst = pl.ds(k * piece, piece), w_part(0, k)
        copies = [
            remote(w_key.at[src, kc], wb.at[dst, :dk], w_sem(slot, k), peer, core, when),
            remote(w_value.at[src, vc], wb.at[dst, dk:], w_sem(slot, k), peer, core, when),
        ]
        start(copies, when)

    def w_relay(slot, k, peer, there, when=None):
        rows = w_part(slot, k)
        start([remote(wb.at[rows], wb.at[rows], w_sem(there, k), peer, core, when)], when)

    def w_wait(slot, k):
        landed(wb.at[w_part(slot, k)], w_sem(slot, k))

    def pass_rows(k):
        return pass_w.at[pl.ds(k * piece, piece)]

    def columns(owner, k):
        return pl.ds(pl.multiple_of((owner * PARTS + k) * cut, cut), cut)

    def rows_of(kind, unit):
        if kind in ("x1", "x2", "x3"):
            chunk = {"x1": 2 + unit // PARTS, "x2": 4, "x3": 5}[kind]
            return chunk * span, span
        chunk = {"a": 6, "b": 7, "c": 8}[kind[1]]
        return chunk * span + (half if kind[0] == "y" else 0), half

    def part(kind, unit, owner):
        low, size = rows_of(kind, unit)
        return xb.at[pl.ds(low, size), columns(owner, unit % PARTS)]

    def sem(table, kind, unit):
        return table.at[KINDS.index(kind), unit]

    def x_own(s, low, size, kind, unit, peer, when=None):
        src = prompt.at[s, pl.ds(low, size), columns(core, unit % PARTS)]
        copy = remote(src, part(kind, unit, core), sem(x_recv, kind, unit), peer, core, when)
        start([copy], when)

    def x_pass(kind, there, unit, peer, when=None):
        copy = remote(
            part(kind, unit, core),
            part(there, unit, core),
            sem(x_recv, there, unit),
            peer,
            core,
            when,
        )
        start([copy], when)

    def only(kind):
        return inner if kind[1] in "bc" else None

    def x_across(kind, unit):
        own = part(kind, unit, core)
        when = only(kind)
        start([remote(own, own, sem(d_recv, kind, unit), me, 1 - core, when)], when)

    def maybe(when, run):
        if when is None:
            run()
        else:
            pl.when(when)(run)

    def x_wait(kind, unit):
        maybe(
            only(kind),
            lambda: landed(part(kind, unit, core), sem(x_recv, kind, unit)),
        )

    def d_wait(kind, unit):
        maybe(
            only(kind),
            lambda: landed(part(kind, unit, 1 - core), sem(d_recv, kind, unit)),
        )

    def go_x(kind, unit):
        x_wait(kind, unit)
        if kind == "x2":
            x_pass("x2", "x3", unit, to_x)
        if kind == "xa":
            x_pass("xa", "ya", unit, to_x, outer if unit >= PARTS // 2 else None)
        if kind == "xc":
            x_pass("xc", "yc", unit, to_x, inner)
        if kind == "x1" and unit >= PARTS:
            k = unit - PARTS
            src = xb.at[pl.ds(3 * span + half, half), columns(core, k)]
            dst = part("yb", k, core)
            start([remote(src, dst, sem(x_recv, "yb", k), to_z, core, outer)], outer)
            if k >= PARTS // 2:
                src = xb.at[pl.ds(3 * span, half), columns(core, k)]
                dst = part("ya", k, core)
                start([remote(src, dst, sem(x_recv, "ya", k), to_z, core, outer)], outer)
        x_across(kind, unit)

    first = core == 0

    def px2(k):
        kc, vc = group_cols(1, 1)
        src, dst = pl.ds(k * piece, piece), pass_rows(k)
        start(
            [
                remote(w_key.at[src, kc], dst.at[:, :dk], w_sem(0, k), to_x, core),
                remote(w_value.at[src, vc], dst.at[:, dk:], w_sem(0, k), to_x, core),
            ]
        )

    def greet():
        @pl.when(inner)
        def _():
            tell(ready, to_z, core)
            tell(ready, to_mid, core)

        pl.semaphore_wait(ready, 1)

    w_gate = jnp.concatenate([w_igate[...], w_fgate[...]], axis=0)
    square = iota((total_heads, total_heads), 0) == iota((total_heads, total_heads), 1)

    def upright(row):
        return jnp.sum(jnp.where(square, row, 0.0), axis=1, keepdims=True)

    bias_in, bias_f = upright(input_bias[...]), upright(forget_bias[...])
    after = (iota((span, span), 0) > iota((span, span), 1)).astype(f32)
    spot_head = iota((total_heads, 128), 0) - core * heads
    spot_lane = iota((total_heads, 128), 1)
    local_head = (spot_head >= 0) & (spot_head < heads)
    def gates():
        for c in own_x:
            c.wait()
        packed = jnp.zeros((1, 128), f32)
        for s in range(seqs):
            both = lax.dot_general(
                w_gate,
                xb[s * span : (s + 1) * span],
                (((1,), (1,)), ((), ())),
                preferred_element_type=f32,
            )
            gate_in = both[:total_heads] + bias_in
            forget = log_sigmoid(both[total_heads:] + bias_f)
            level = gate_in + jnp.dot(forget, after, precision=HIGH, preferred_element_type=f32)
            top = jnp.max(level, axis=1, keepdims=True)
            total = jnp.sum(forget, axis=1, keepdims=True)
            part_w = jnp.exp(level - top) * key_scale
            gate_w[0, s * heads : (s + 1) * heads, :span] = jnp.where(
                first, part_w[:heads], part_w[heads : 2 * heads]
            )
            at = spot_lane - s * heads
            packed = packed + jnp.sum(
                jnp.where(local_head & (at == spot_head), total, 0.0)
                + jnp.where(local_head & (at - seqs * heads == spot_head), top, 0.0),
                axis=0,
                keepdims=True,
            )
        stat[me] = jnp.broadcast_to(packed, (8, 128))
        for c in own_w:
            c.wait()

    def tell_all():
        for off in range(count - 1, 0, -1):
            peer = place(*bits(off))
            start([remote(stat.at[me], stat.at[me], s_recv, peer, core)])
        for block, peer in ((1, to_x), (2, to_z), (3, place(0, 1, 0, 1))):
            start([remote(gate_w.at[0], gate_w.at[block], g_recv.at[block], peer, core)])
        for block, peer in ((4, to_mid), (5, place(1, 1, 0, 1))):
            copy = remote(
                gate_w.at[0], gate_w.at[block], g_recv.at[block], peer, core, inner
            )
            start([copy], inner)

    def choose(i, values):
        out = jnp.int32(values[0])
        for k, v in enumerate(values[1:], 1):
            out = jnp.where(i == k, v, out)
        return out

    def multiply(low, size, slots):
        width_in = 4 if len(slots) % 4 == 0 else 2

        def step(i, carry):
            out = None
            for off in range(width_in):
                rows = w_rows(choose(i, slots[off::width_in]))
                piece = jnp.dot(
                    xb[pl.ds(low, size), rows], wb[rows], preferred_element_type=f32
                )
                out = piece if out is None else out + piece
            acc[pl.ds(low, size)] += out
            return carry

        lax.fori_loop(0, len(slots) // width_in, step, 0)

    def multiply_part(low, size, k):
        out = None
        for owner in range(2):
            cols = slice((owner * PARTS + k) * cut, (owner * PARTS + k + 1) * cut)
            piece = jnp.dot(xb[low : low + size, cols], wb[cols], preferred_element_type=f32)
            out = piece if out is None else out + piece
        acc[low : low + size] += out

    def zero(i, carry):
        acc[pl.ds(pl.multiple_of(i * span, span), span)] = jnp.zeros((span, dk + dv), f32)
        return carry

    lax.fori_loop(0, 9, zero, 0)

    eye = (iota((span, span), 0) == iota((span, span), 1)).astype(f32)
    here = iota((span, seqs * heads), 1)
    chip = iota((count, seqs * heads), 0)
    lane16 = iota((count, seqs * heads), 1)

    def weigh():
        landed(stat.at[pl.ds(0, count - 1)], s_recv)
        table = jnp.concatenate([stat[c, 0:1] for c in range(count)], axis=0)
        beyond = (iota((count, count), 1) > iota((count, count), 0)).astype(f32)
        later = jnp.dot(beyond, table, precision=HIGH, preferred_element_type=f32)
        lift = later[:, : seqs * heads] + table[:, seqs * heads : 2 * seqs * heads]
        highest = jnp.max(lift, axis=0, keepdims=True)
        factor = jnp.exp(lift - highest)
        weight[8 * span : 9 * span] = jnp.zeros((span, 128), f32)

        def column(block, s):
            turned = lax.dot_general(
                eye,
                gate_w[block][:, :span],
                (((1,), (1,)), ((), ())),
                precision=HIGH,
                preferred_element_type=f32,
            )
            dh, pos = (0, block) if block < 4 else (1, 2 + block % 2)
            lane = s * heads + mine
            hit = (chip == place(dh, pos // 2, 0, pos % 2)) & (lane16 == lane)
            scale = jnp.sum(jnp.where(hit, factor, 0.0), keepdims=True)
            one = jnp.sum(jnp.where(here == lane, turned, 0.0), axis=1, keepdims=True)
            return jnp.broadcast_to(one * scale, (span, 128))

        for block in range(4):
            if block:
                landed(gate_w.at[block], g_recv.at[block])
            weight[pl.ds((2 * block if block < 2 else 2 + block) * span, span)] = column(block, 0)
            late = column(block, 1)
            if block < 2:
                weight[pl.ds((2 * block + 1) * span, span)] = late
            else:
                for chunk in (6, 7):
                    low = chunk * span + (block - 2) * half
                    weight[pl.ds(low, half)] = late[(chunk - 6) * half : (chunk - 5) * half]

        @pl.when(inner)
        def _():
            for block in (4, 5):
                landed(gate_w.at[block], g_recv.at[block])
                low = 8 * span + (block - 4) * half
                weight[pl.ds(low, half)] = column(block, 1)[half:]

        return highest

    to_chunk = (0, 4, 1, 5, 2, 3, 6, 7, 8)

    def finish(chunk):
        rows = slice(chunk * span, (chunk + 1) * span)
        to = slice(to_chunk[chunk] * span, (to_chunk[chunk] + 1) * span)
        keys = acc[rows, :dk].astype(bf16).astype(f32)
        decay[to] = (weight[rows, 0:1] * keys).astype(bf16)
        vals[to] = acc[rows, dk:].astype(bf16)

    pick = iota((heads, dk), 0) == mine

    def out_rows(chip):
        return pl.ds(pl.multiple_of(chip * rows_out, rows_out), rows_out)

    def reduce(s):
        span_rows = slice(0, 4 * span) if s == 0 else slice(4 * span, 9 * span)
        d = decay[span_rows]
        ones = jnp.ones((8, d.shape[0]), bf16)
        sums = lax.dot_general(
            d, vals[span_rows], (((0,), (0,)), ((), ())), preferred_element_type=f32
        )
        high = sums.astype(bf16)
        if s == 0:
            for block in range(count // 2):
                low = (block // 2) * 2 * rows_out
                state[block % 2, low : low + 2 * rows_out] = high[
                    block * 2 * rows_out : (block + 1) * 2 * rows_out
                ]
            start([remote(state.at[1 - y], y_in, y_recv.at[0], to_y, core)])
        else:
            late_state[...] = high
            for off in range(count - 1, 0, -1):
                peer = place(*bits(off))
                src = late_state.at[out_rows(peer)]
                start([remote(src, rmem.at[1, me], m_recv.at[1], peer, core)])
        low = (sums - high.astype(f32)).astype(bf16)
        norms = jnp.dot(ones, d, preferred_element_type=f32)
        query = jnp.sum(
            jnp.where(pick, new_query[s].astype(f32), 0.0), axis=0, keepdims=True
        )
        wide = jnp.broadcast_to(query, (8, dk)).astype(bf16)
        seen = jnp.dot(wide, high, preferred_element_type=f32) + jnp.dot(
            wide, low, preferred_element_type=f32
        )
        for k in range(dv // 128):
            aux[s, k : k + 1] = seen[0:1, k * 128 : (k + 1) * 128]
        for k in range(dk // 128):
            aux[s, 4 + k : 5 + k] = norms[0:1, k * 128 : (k + 1) * 128]
        dot_norm = jnp.sum(query * norms[0:1], axis=1, keepdims=True)
        aux[s, 6:8] = jnp.broadcast_to(dot_norm, (2, 128))
        if s == 0:
            start([remote(aux.at[0], y_aux, y_recv.at[1], to_y, core)])
        else:
            for off in range(count - 1, 0, -1):
                peer = place(*bits(off))
                start([remote(aux.at[1], raux.at[1, me], a_recv.at[1], peer, core)])
            rmem[1, me] = late_state[out_rows(me)]
            raux[1, me] = aux[1]

    spot8 = (zh * 2 + zl) * 2 + x

    def reduce_on():
        landed(y_in, y_recv.at[0])
        pair_state[...] = (state[y].astype(f32) + y_in[...].astype(f32)).astype(bf16)
        landed(y_aux, y_recv.at[1])
        pair_aux[...] = aux[0] + y_aux[...]
        for off in range(count // 2 - 1, 0, -1):
            dh, dl, dx = off // 4, (off // 2) % 2, off % 2
            peer = place(dh, dl, 0, dx)
            spot = (flip(zh, dh) * 2 + flip(zl, dl)) * 2 + flip(x, dx)
            src = pair_state.at[out_rows(spot)]
            start([remote(src, rmem.at[0, spot8], m_recv.at[0], peer, core)])
            start([remote(pair_aux, raux.at[0, spot8], a_recv.at[0], peer, core)])
        rmem[0, spot8] = pair_state[out_rows(spot8)]
        raux[0, spot8] = pair_aux[...]

    streams = {"px": (0, 1, to_x, 1), "yown": (0, 0, to_y, 2), "near": (1, 0, to_z, 4)}
    greeted = False
    highest = None
    for name, *arg in SCHEDULE:
        if name in streams:
            w_own(*streams[name], arg[0])
        elif name == "px2":
            px2(arg[0])
        elif name == "far":
            if not greeted:
                greet()
            greeted = True
            w_own(0, 0, to_far, 8, arg[0])
        elif name == "mid":
            w_own(1, 0, to_mid, 12, arg[0], inner)
        elif name == "gates":
            gates()
        elif name == "tell_all":
            tell_all()
        elif name == "tx":
            x_own(arg[0] // PARTS, 0, span, "x1", arg[0], to_x)
        elif name == "tz":
            x_own(0, 0, span, "x2", arg[0], to_z)
        elif name == "ta":
            x_own(1, 0, half, "xa", arg[0], to_z)
        elif name == "tb":
            x_own(1, half, half, "xb", arg[0], to_z, outer)
            x_own(1, half, half, "xc", arg[0], to_mid, inner)
        elif name == "w":
            slot, k = arg
            w_wait(slot, k)
            if slot == 1:
                w_relay(1, k, to_far, 9)
            if slot % 4 < 2:
                w_relay(slot, k, to_y, slot + 2)
            if slot in (4, 5):
                w_relay(slot, k, to_far, slot + 8, inner)
        elif name == "p":
            k = arg[0]
            landed(pass_rows(k), w_sem(0, k))
            dst = wb.at[w_part(1, k)]
            start([remote(pass_rows(k), dst, w_sem(5, k), to_z, core)])
        elif name == "pm":
            k = arg[0]
            dst = wb.at[w_part(1, k)]
            start([remote(pass_rows(k), dst, w_sem(13, k), to_mid, core, inner)], inner)
        elif name in KINDS:
            go_x(name, arg[0])
        elif name == "d":
            kind, low = arg
            for unit in range(low, low + PARTS):
                d_wait(kind, unit)
        elif name == "mm":
            low, chunks, slots = arg
            maybe(
                inner if low >= 7 else None,
                lambda: multiply(low * span, chunks * span, slots),
            )
        elif name == "d1":
            d_wait(*arg)
        elif name == "mma":
            low, chunks, k = arg
            maybe(
                inner if low >= 7 else None,
                lambda: multiply_part(low * span, chunks * span, k),
            )
        elif name == "weigh":
            highest = weigh()
        elif name == "finish":
            for chunk in arg:
                finish(chunk)
        elif name == "reduce":
            reduce(arg[0])
        elif name == "reduce_on":
            reduce_on()

    def stack(ref):
        return jnp.concatenate([ref[s].astype(f32) for s in range(seqs)], axis=0)

    queries = stack(new_query)
    own = jnp.sum(queries * stack(new_key), axis=1, keepdims=True) * key_scale
    own_head = iota((seqs * heads, heads), 0) % heads == iota((seqs * heads, heads), 1)

    def gate_column(block):
        wide = jnp.concatenate(
            [jnp.broadcast_to(block[s : s + 1], (heads, heads)) for s in range(seqs)], axis=0
        )
        return jnp.sum(jnp.where(own_head, wide, 0.0), axis=1, keepdims=True)

    gate_in, gate_f = gate_column(new_gates[0]), log_sigmoid(gate_column(new_gates[1]))
    token_values = stack(new_value)
    top = upright(highest)
    max_out[...] = top

    read_rows, norm_rows, dot_rows = [], [], []
    for s in range(seqs):
        peers = count // 2 - 1 if s == 0 else count - 1
        landed(rmem.at[s, pl.ds(0, peers)], m_recv.at[s])
        landed(raux.at[s, pl.ds(0, peers)], a_recv.at[s])
        for h in range(heads):
            if s == 0:
                srcs = [(a * 2 + h // 2) * 2 + h % 2 for a in range(2)]
            else:
                srcs = [
                    (a * 2 + h // 2) * 4 + b * 2 + h % 2 for a in range(2) for b in range(2)
                ]
            mem = rmem[s, srcs[0]].astype(f32)
            both = raux[s, srcs[0]]
            for src in srcs[1:]:
                mem = mem + rmem[s, src].astype(f32)
                both = both + raux[s, src]
            memory_out[s, h] = mem.astype(bf16)
            read_rows.append(
                jnp.concatenate([both[k : k + 1] for k in range(dv // 128)], 1)
            )
            norm_rows.append(
                jnp.concatenate([both[4 + k : 5 + k] for k in range(dk // 128)], 1)
            )
            dot_rows.append(both[6:7, 0:1])
    query_state = jnp.concatenate(read_rows, axis=0)
    norm_all = jnp.concatenate(norm_rows, axis=0)
    query_norm = jnp.concatenate(dot_rows, axis=0)
    take = (
        iota((dk, rows_out), 0) == me * rows_out + iota((dk, rows_out), 1)
    ).astype(f32)
    norm_out[...] = jnp.dot(norm_all, take, precision=HIGH, preferred_element_type=f32)
    mixed = jnp.maximum(gate_f + top, gate_in)
    carried = jnp.exp(gate_f + top - mixed)
    fresh = jnp.exp(gate_in - mixed)
    numer = carried * query_state + (fresh * own) * token_values
    denom = carried * query_norm + fresh * own
    read_out[...] = (numer / jnp.maximum(jnp.abs(denom), 1.0)).astype(bf16)
    for copy, when in sent:
        if when is None:
            copy.wait_send()
        else:
            pl.when(when)(copy.wait_send)


def hand_on(memory, norm, top, read, memory_out, norm_out, max_out, read_out):
    seqs, heads = max_out.shape
    memory_out[...] = memory[...]
    at = lax.broadcasted_iota(jnp.int32, (seqs * heads, heads), 0)
    to = lax.broadcasted_iota(jnp.int32, (seqs * heads, heads), 1)
    wide = read[...].astype(jnp.float32)
    for s in range(seqs):
        rows = slice(s * heads, (s + 1) * heads)
        norm_out[s] = norm[rows]
        read_out[s] = wide[rows].astype(jnp.bfloat16)
        max_out[s : s + 1] = jnp.sum(
            jnp.where(at == s * heads + to, top[...], 0.0), axis=0, keepdims=True
        )


def by_head(
    prompt,
    w_key,
    w_value,
    w_igate,
    w_fgate,
    input_bias,
    forget_bias,
    new_query,
    new_key,
    new_value,
    new_gates,
):
    count = lax.axis_size("sp")
    seqs, span, width = prompt.shape
    depth = w_key.shape[0]
    heads, dk = new_query.shape[1:]
    dv = new_value.shape[2]
    rows = seqs * span
    vmem = pl.BlockSpec(memory_space=pltpu.VMEM)
    hbm = pl.BlockSpec(memory_space=pl.ANY)
    dma = pltpu.SemaphoreType.DMA
    memory, norm, top, read = pl.pallas_call(
        kernel,
        out_shape=(
            jax.ShapeDtypeStruct((seqs, heads, dk // count, dv), jnp.bfloat16),
            jax.ShapeDtypeStruct((seqs * heads, dk // count), jnp.float32),
            jax.ShapeDtypeStruct((seqs * heads, 1), jnp.float32),
            jax.ShapeDtypeStruct((seqs * heads, dv), jnp.bfloat16),
        ),
        in_specs=[hbm, hbm, hbm] + [vmem] * 8,
        out_specs=(vmem, vmem, vmem, vmem),
        scratch_shapes=[
            pltpu.VMEM((9 * span, width), jnp.bfloat16),
            pltpu.VMEM((width, dk + dv), jnp.bfloat16),
            pltpu.VMEM((depth, dk + dv), jnp.bfloat16),
            pltpu.VMEM((9 * span, dk + dv), jnp.float32),
            pltpu.VMEM((9 * span, dk), jnp.bfloat16),
            pltpu.VMEM((9 * span, dv), jnp.bfloat16),
            pltpu.VMEM((9 * span, 128), jnp.float32),
            pltpu.VMEM((6, 8, 256), jnp.float32),
            pltpu.VMEM((count, 8, 128), jnp.float32),
            pltpu.VMEM((2, dk // 2, dv), jnp.bfloat16),
            pltpu.VMEM((dk, dv), jnp.bfloat16),
            pltpu.VMEM((dk // 2, dv), jnp.bfloat16),
            pltpu.VMEM((dk // 2, dv), jnp.bfloat16),
            pltpu.VMEM((seqs, 8, 128), jnp.float32),
            pltpu.VMEM((8, 128), jnp.float32),
            pltpu.VMEM((8, 128), jnp.float32),
            pltpu.VMEM((seqs, count, dk // count, dv), jnp.bfloat16),
            pltpu.VMEM((seqs, count, 8, 128), jnp.float32),
            dma((4,)),
            pltpu.SemaphoreType.REGULAR,
            dma((SENDS,)),
            dma((len(KINDS), 2 * PARTS)),
            dma((len(KINDS), 2 * PARTS)),
            dma((32,)),
            dma((6,)),
            dma,
            dma((2,)),
            dma((seqs,)),
            dma((seqs,)),
        ],
        compiler_params=pltpu.CompilerParams(
            collective_id=0, has_side_effects=True, vmem_limit_bytes=60 * 1024 * 1024
        ),
    )(
        prompt,
        w_key,
        w_value,
        w_igate.T,
        w_fgate.T,
        input_bias[None],
        forget_bias[None],
        new_query,
        new_key,
        new_value,
        new_gates,
    )
    return pl.pallas_call(
        hand_on,
        out_shape=(
            jax.ShapeDtypeStruct((seqs, heads, dk // count, dv), jnp.bfloat16),
            jax.ShapeDtypeStruct((seqs, heads, dk // count), jnp.float32),
            jax.ShapeDtypeStruct((seqs, heads), jnp.float32),
            jax.ShapeDtypeStruct((seqs, heads, dv), jnp.bfloat16),
        ),
        in_specs=[vmem] * 4,
        out_specs=(vmem,) * 4,
    )(memory, norm, top, read)


def chosen(*args):
    prompt, new_query, new_value = args[0], args[7], args[9]
    heads = new_query.shape[1]
    count = lax.axis_size("sp")
    fits = (
        lax.axis_size("tp") == 2
        and heads == 4
        and count == 16
        and prompt.shape[0] == 2
        and new_query.shape[2] == 256
        and new_value.shape[2] == 512
    )
    return by_head(*args) if fits else per_device(*args)


def entering(value, axis, join, neutral):
    count, mine = (lax.axis_size(axis), lax.axis_index(axis))
    pieces = lax.all_gather(value, axis)
    pieces = pieces[::-1]
    mine = count - 1 - mine
    so_far = jnp.full_like(value, 0) + jnp.asarray(neutral, value.dtype)

    def turn(position, so_far):
        longer = join(so_far, pieces[position])
        return jnp.where(position < mine, longer, so_far)

    return lax.fori_loop(0, count - 1, turn, so_far)


def add_pair(earlier, later):
    return earlier + later


def per_device(
    prompt,
    w_key,
    w_value,
    w_igate,
    w_fgate,
    input_bias,
    forget_bias,
    new_query,
    new_key,
    new_value,
    new_gates,
):
    seq_count, span_len, model_width = prompt.shape
    local_heads = new_query.shape[1]
    key_size = new_query.shape[2]
    value_size = new_value.shape[2]
    key_scale = key_size ** (-0.5)
    token_rows = prompt.reshape(seq_count * span_len, model_width)
    whole_key, whole_value = (
        lax.all_gather(w_key, "sp", axis=0, tiled=True),
        lax.all_gather(w_value, "sp", axis=0, tiled=True),
    )
    key_rows = jnp.dot(token_rows, whole_key, preferred_element_type=jnp.float32).astype(
        jnp.bfloat16
    )
    value_rows = jnp.dot(token_rows, whole_value, preferred_element_type=jnp.float32).astype(
        jnp.bfloat16
    )
    head_start = lax.axis_index("tp") * local_heads
    input_all = jnp.dot(token_rows, w_igate, preferred_element_type=jnp.float32) + input_bias
    forget_all = jnp.dot(token_rows, w_fgate, preferred_element_type=jnp.float32) + forget_bias
    input_gate = lax.dynamic_slice_in_dim(input_all, head_start, local_heads, 1).reshape(
        seq_count, span_len, local_heads
    )
    log_forget = jax.nn.log_sigmoid(
        lax.dynamic_slice_in_dim(forget_all, head_start, local_heads, 1)
    ).reshape(seq_count, span_len, local_heads)
    block_total = jnp.sum(log_forget, axis=1)
    forget_after = block_total[:, None] - jnp.cumsum(log_forget, axis=1)
    log_weight = forget_after + input_gate
    block_max = jnp.max(log_weight, axis=1)
    key_blocks = key_rows.reshape(seq_count, span_len, local_heads, key_size).astype(jnp.float32)
    decayed = (jnp.exp(log_weight - block_max[:, None])[..., None] * key_scale * key_blocks).astype(
        jnp.bfloat16
    )
    value_blocks = value_rows.reshape(seq_count, span_len, local_heads, value_size)
    block_norm = jnp.sum(decayed.astype(jnp.float32), axis=1)
    later_total = entering(block_total, "sp", add_pair, jnp.zeros_like(block_total))
    block_lift = later_total + block_max
    global_max = lax.pmax(block_lift, "sp")
    factor = jnp.exp(block_lift - global_max)
    scaled_norm = factor[:, :, None] * block_norm
    query_full = new_query.astype(jnp.float32)
    block_state = jnp.einsum(
        "sthk,sthv->shkv", decayed, value_blocks, preferred_element_type=jnp.float32
    )
    scaled_state = factor[:, :, None, None] * block_state
    memory_rows, norm_rows = (
        lax.psum_scatter(scaled_state, "sp", scatter_dimension=2, tiled=True),
        lax.psum_scatter(scaled_norm, "sp", scatter_dimension=2, tiled=True),
    )
    token_score = jnp.einsum(
        "shk,sthk->sth", new_query, decayed, preferred_element_type=jnp.float32
    )
    score_high = token_score.astype(jnp.bfloat16)
    score_low = (token_score - score_high.astype(jnp.float32)).astype(jnp.bfloat16)
    weighted = jnp.einsum(
        "sth,sthv->shv", score_high, value_blocks, preferred_element_type=jnp.float32
    )
    weighted = weighted + jnp.einsum(
        "sth,sthv->shv", score_low, value_blocks, preferred_element_type=jnp.float32
    )
    partial_state = factor[..., None] * weighted
    partial_norm = jnp.sum(query_full * scaled_norm, axis=-1)
    query_state, query_norm = lax.psum((partial_state, partial_norm), "sp")
    forget_new = jax.nn.log_sigmoid(new_gates[1])
    input_new = new_gates[0]
    mixed = jnp.maximum(forget_new + global_max, input_new)
    carried = jnp.exp(forget_new + global_max - mixed)
    fresh = jnp.exp(input_new - mixed)
    own_score = jnp.sum(query_full * new_key.astype(jnp.float32), axis=-1) * key_scale
    numer = carried[..., None] * query_state + (fresh * own_score)[..., None] * new_value.astype(
        jnp.float32
    )
    denom = carried * query_norm + fresh * own_score
    first_read = (numer / jnp.maximum(jnp.abs(denom), 1.0)[..., None]).astype(jnp.bfloat16)
    return (memory_rows.astype(jnp.bfloat16), norm_rows, global_max, first_read)


def solution(mesh):
    placed = (
        P(None, "sp", None),
        P("sp", "tp"),
        P("sp", "tp"),
        P(),
        P(),
        P(),
        P(),
        P(None, "tp", None),
        P(None, "tp", None),
        P(None, "tp", None),
        P(None, None, "tp"),
    )
    return jax.shard_map(
        chosen,
        mesh=mesh,
        in_specs=placed,
        out_specs=(
            P(None, "tp", "sp", None),
            P(None, "tp", "sp"),
            P(None, "tp"),
            P(None, "tp", None),
        ),
        check_vma=False,
    )
```
